32 devices in a mesh: tp: 8 (over z, y), dp: 4 (over x, core).
Axes of the slice: x: 2, y: 2, z: 4, core: 2. Of those that a mesh axis runs over, the one named last changes fastest.
Arguments:
- tokens: bfloat16 [192, 8448], P('dp', 'tp'), may hold values from -6 to 6
- gains: float32 [2, 8448], replicated, may hold values from 0.1 to 1.9
- w_input: bfloat16 [2, 8448, 12288], P(None, 'dp', 'tp'), may hold values from -0.0625 to 0.0625
- w_gating: bfloat16 [2, 8448, 12288], P(None, 'dp', 'tp'), may hold values from -0.0625 to 0.0625
- w_output: bfloat16 [2, 12288, 8448], P(None, 'tp'), may hold values from -0.21875 to 0.21875
- decay_rate: float32 [2, 768, 64], P(None, 'tp'), may hold values from 0.05 to 2
- frequency: float32 [2, 768, 64], P(None, 'tp'), may hold values from -3 to 3
- log_step: float32 [2, 768], P(None, 'tp'), may hold values from -2.3 to 0
- in_real: float32 [2, 768, 64, 16], P(None, 'tp'), may hold values from -1 to 1
- in_imag: float32 [2, 768, 64, 16], P(None, 'tp'), may hold values from -1 to 1
- readout_real_matrix: float32 [2, 768, 16, 64], P(None, 'tp'), may hold values from -0.5 to 0.5
- readout_imag_matrix: float32 [2, 768, 16, 64], P(None, 'tp'), may hold values from -0.5 to 0.5
- skip_gain: float32 [2, 12288], P(None, 'tp'), may hold values from -4 to 4
- state_real: float32 [2, 192, 768, 64], P(None, 'dp', 'tp'), may hold values from -6 to 6
- state_imag: float32 [2, 192, 768, 64], P(None, 'dp', 'tp'), may hold values from -6 to 6
Outputs:
- mixed: bfloat16 [192, 8448], P('dp', 'tp')
- next_real: float32 [2, 192, 768, 64], P(None, 'dp', 'tp')
- next_imag: float32 [2, 192, 768, 64], P(None, 'dp', 'tp')
The draws below stay inside these ranges and needn't reach their ends.
All inputs are finite; a program needn't handle non-finite values.
Results may differ from the reference program's by a relative error of at most 0.008.
Values may be sent and summed in bfloat16 or wider, within the bound.
A program may use at most 256 MiB of HBM per device.

```python
import math
import jax
import jax.numpy as jnp
from jax import lax

D = 8448
G = 768
GS = 16
P_SIZE = 64
LAYERS = 2
BATCH = 192
W = 12288


def with_spikes(drawn, stream_key, source, target, shards_of, factor):
    owner, partner = [(jnp.arange(drawn.shape[position]) // (drawn.shape[position] // shards_of)).reshape([-1 if axis == position else 1 for axis in range(drawn.ndim)]) for position in (source, target)]
    chosen = jax.random.permutation(stream_key, shards_of)[partner]
    strong = (owner == chosen) | (owner == (partner + shards_of // 2) % shards_of)
    return jnp.where(strong, factor * drawn, drawn)


def steps_of(stream_key, shape, split, low, largest):
    def one(dim, shards_of):
        steps = jax.random.uniform(jax.random.fold_in(jax.random.fold_in(stream_key, 6), dim), (shards_of,), jnp.float32, low / len(split), largest / len(split))
        return jnp.repeat(jnp.exp(steps), shape[dim] // shards_of).reshape((-1,) + (1,) * (len(shape) - dim - 1))

    gain = one(*split[0])
    for cut in split[1:]:
        gain = gain * one(*cut)
    return gain


def gaussian(stream_key, shape, width, bound, pieces=(), dtype=jnp.bfloat16):
    entries = width * jax.random.normal(stream_key, shape, jnp.float32)
    if pieces:
        entries = entries * steps_of(stream_key, shape, pieces, -0.22, 0.18)
    return jnp.clip(entries, -bound, bound).astype(dtype)


def noise_with(rng, dims, width, bound, shards, heavy, kind=jnp.bfloat16):
    entries = width * jax.random.normal(rng, dims, jnp.float32)
    if shards:
        entries = entries * steps_of(rng, dims, shards, -0.22, 0.18)
    return jnp.clip(with_spikes(entries, jax.random.fold_in(rng, 3), *heavy), -bound, bound).astype(kind)


def setup_inputs(seed: int = 0) -> dict:
    streams_of = jax.random.split(jax.random.key(seed), 16)
    return {
        "tokens": gaussian(streams_of[0], (BATCH, D), 1.0, 6.0, ((0, 4), (1, 8))),
        "gains": jnp.clip(1.0 + 0.18 * jax.random.normal(streams_of[1], (LAYERS, D), jnp.float32), 0.1, 1.9),
        "w_input": gaussian(streams_of[2], (LAYERS, D, W), D ** -0.5, 0.0625, ((1, 4), (2, 8))),
        "w_gating": gaussian(streams_of[3], (LAYERS, D, W), D ** -0.5, 0.0625, ((1, 4), (2, 8))),
        "w_output": noise_with(streams_of[4], (LAYERS, W, D), (W // 8) ** -0.5, 0.21875, ((1, 8),), (1, 2, 8, 2.0)),
        "decay_rate": jnp.clip(jnp.exp(math.log(2.0) - 3.6888794 * jax.random.uniform(streams_of[5], (LAYERS, G, P_SIZE), jnp.float32) ** steps_of(streams_of[5], (LAYERS, G, P_SIZE), ((1, 8),), -0.2, 0.2)), 0.05, 2.0),
        "frequency": jnp.clip(jax.random.uniform(streams_of[6], (LAYERS, G, P_SIZE), jnp.float32, -3.0, 3.0) * steps_of(streams_of[6], (LAYERS, G, P_SIZE), ((1, 8),), -0.4, 0.0), -3.0, 3.0),
        "log_step": jnp.clip(-2.3 + 2.3 * jax.random.uniform(streams_of[7], (LAYERS, G), jnp.float32) ** steps_of(streams_of[7], (LAYERS, G), ((1, 8),), -0.2, 0.2), -2.3, 0.0),
        "in_real": gaussian(streams_of[8], (LAYERS, G, P_SIZE, GS), (2 * GS) ** -0.5, 1.0, ((1, 8),), jnp.float32),
        "in_imag": gaussian(streams_of[9], (LAYERS, G, P_SIZE, GS), (2 * GS) ** -0.5, 1.0, ((1, 8),), jnp.float32),
        "readout_real_matrix": gaussian(streams_of[10], (LAYERS, G, GS, P_SIZE), (2 * P_SIZE) ** -0.5, 0.5, ((1, 8),), jnp.float32),
        "readout_imag_matrix": gaussian(streams_of[11], (LAYERS, G, GS, P_SIZE), (2 * P_SIZE) ** -0.5, 0.5, ((1, 8),), jnp.float32),
        "skip_gain": gaussian(streams_of[12], (LAYERS, W), 1.0, 4.0, ((1, 8),), jnp.float32),
        "state_real": gaussian(streams_of[13], (LAYERS, BATCH, G, P_SIZE), 1.0, 6.0, ((1, 4), (2, 8)), jnp.float32),
        "state_imag": gaussian(streams_of[14], (LAYERS, BATCH, G, P_SIZE), 1.0, 6.0, ((1, 4), (2, 8)), jnp.float32),
    }


PRECISION_LEVEL = lax.Precision.HIGHEST

def reference(tokens, gains, w_input, w_gating, w_output, decay_rate, frequency, log_step, in_real, in_imag, readout_real_matrix, readout_imag_matrix, skip_gain, state_real, state_imag):
    x = tokens
    outs_re = []
    outs_im = []
    batch = x.shape[0]
    for layer_params in range(LAYERS):
        xf = x.astype(jnp.float32)
        meansq = lax.optimization_barrier(jnp.mean(xf * xf, axis=1, keepdims=True))
        inverse = lax.rsqrt(meansq + 1e-06)
        scaled = (xf * gains[layer_params][None, :]).astype(jnp.bfloat16)
        drive = jnp.dot(scaled, w_input[layer_params], preferred_element_type=jnp.float32) * inverse
        gate = jnp.dot(scaled, w_gating[layer_params], preferred_element_type=jnp.float32) * inverse
        step = jnp.exp(log_step[layer_params])[:, None]
        lam_re = -decay_rate[layer_params]
        lam_im = frequency[layer_params]
        magnitude = jnp.exp(lam_re * step)
        angle = lam_im * step
        abar_re = magnitude * jnp.cos(angle)
        abar_im = magnitude * jnp.sin(angle)
        denom = lam_re * lam_re + lam_im * lam_im
        num_re = abar_re - 1.0
        zoh_re = (num_re * lam_re + abar_im * lam_im) / denom
        zoh_im = (abar_im * lam_re - num_re * lam_im) / denom
        bbar_re = zoh_re[..., None] * in_real[layer_params] - zoh_im[..., None] * in_imag[layer_params]
        bbar_im = zoh_re[..., None] * in_imag[layer_params] + zoh_im[..., None] * in_real[layer_params]
        grouped = drive.reshape(batch, G, GS)
        push_re = jnp.einsum('bgc,gpc->bgp', grouped, bbar_re, precision=PRECISION_LEVEL)
        push_im = jnp.einsum('bgc,gpc->bgp', grouped, bbar_im, precision=PRECISION_LEVEL)
        old_re = state_real[layer_params]
        old_im = state_imag[layer_params]
        updated_real = abar_re[None] * old_re - abar_im[None] * old_im + push_re
        updated_imag = abar_re[None] * old_im + abar_im[None] * old_re + push_im
        readout_output = jnp.einsum('zju,jiu->zji', updated_real, readout_real_matrix[layer_params], precision=PRECISION_LEVEL) - jnp.einsum('zju,jiu->zji', updated_imag, readout_imag_matrix[layer_params], precision=PRECISION_LEVEL)
        readout_output = readout_output + skip_gain[layer_params].reshape(G, GS)[None] * grouped
        gated = (jax.nn.gelu(readout_output.reshape(batch, G * GS)) * jax.nn.sigmoid(gate)).astype(jnp.bfloat16)
        branch = jnp.dot(gated, w_output[layer_params], preferred_element_type=jnp.float32)
        x = (xf + branch).astype(jnp.bfloat16)
        outs_re.append(updated_real)
        outs_im.append(updated_imag)
    return (x, jnp.stack(outs_re, axis=0), jnp.stack(outs_im, axis=0))
```

```python
import functools

import jax
import jax.numpy as jnp
from jax import lax
from jax.experimental import pallas as pl
from jax.experimental.pallas import tpu as pltpu
from jax.sharding import PartitionSpec as P

GS = 16
LAYERS = 2
MESH = pl.DeviceIdType.MESH
ANY = pl.BlockSpec(memory_space=pl.ANY)


def exchange_kernel(axis, n, count, *refs):
    ins, outs = refs[:count], refs[count : 2 * count]
    send, recv, local = refs[2 * count :]
    me = lax.axis_index(axis)
    barrier = pltpu.get_barrier_semaphore()
    for i in range(1, n):
        pl.semaphore_signal(
            barrier, inc=1, device_id={axis: lax.rem(me + i, n)}, device_id_type=MESH
        )
    own = [
        pltpu.make_async_copy(ins[k].at[me], outs[k].at[me], local.at[k]) for k in range(count)
    ]
    for copy in own:
        copy.start()
    pl.semaphore_wait(barrier, n - 1)
    copies = []
    for i in range(1, n):
        peer = lax.rem(me + i, n)
        for k in range(count):
            copy = pltpu.make_async_remote_copy(
                src_ref=ins[k].at[peer],
                dst_ref=outs[k].at[me],
                send_sem=send.at[k, i],
                recv_sem=recv.at[k, i],
                device_id={axis: peer},
                device_id_type=MESH,
            )
            copy.start()
            copies.append((i, k, copy))
    for copy in own:
        copy.wait()
    for i, k, copy in copies:
        copy.wait_send()
        source = lax.rem(me + n - i, n)
        pltpu.make_async_remote_copy(
            src_ref=ins[k].at[source],
            dst_ref=outs[k].at[source],
            send_sem=send.at[k, i],
            recv_sem=recv.at[k, i],
            device_id={axis: source},
            device_id_type=MESH,
        ).wait_recv()


def exchange(arrays, axis, n, ident):
    count = len(arrays)
    return pl.pallas_call(
        functools.partial(exchange_kernel, axis, n, count),
        out_shape=[jax.ShapeDtypeStruct(a.shape, a.dtype) for a in arrays],
        in_specs=[ANY] * count,
        out_specs=[ANY] * count,
        scratch_shapes=[
            pltpu.SemaphoreType.DMA((count, n)),
            pltpu.SemaphoreType.DMA((count, n)),
            pltpu.SemaphoreType.DMA((count,)),
        ],
        compiler_params=pltpu.CompilerParams(collective_id=ident, has_side_effects=True),
        name=f"exchange_{axis}_{ident}",
    )(*arrays)


def gather_kernel(tp, dp, x_ref, out_ref, send, recv):
    q = tp // dp
    t = lax.axis_index("tp")
    d = lax.axis_index("dp")
    group = t // q
    slot = lax.rem(t, q) * dp + d
    barrier = pltpu.get_barrier_semaphore()
    for h in range(q):
        for r in range(dp):
            source = d * q + h
            pl.semaphore_signal(
                barrier, inc=1, device_id={"tp": source, "dp": r}, device_id_type=MESH
            )

    pl.semaphore_wait(barrier, tp)

    def remote(i, index):
        return pltpu.make_async_remote_copy(
            src_ref=x_ref,
            dst_ref=out_ref.at[index],
            send_sem=send.at[i],
            recv_sem=recv.at[index],
            device_id={"tp": lax.rem(t + i, tp), "dp": group},
            device_id_type=MESH,
        )

    home = group == d

    @pl.when(home)
    def _():
        pltpu.make_async_copy(x_ref, out_ref.at[slot], recv.at[slot]).start()

    @pl.when(jnp.logical_not(home))
    def _():
        remote(0, slot).start()

    for i in range(1, tp):
        remote(i, slot).start()
    for i in range(1, tp):
        remote(i, slot).wait_send()

    @pl.when(jnp.logical_not(home))
    def _():
        remote(0, slot).wait_send()

    for index in range(tp):
        pltpu.make_async_copy(x_ref, out_ref.at[index], recv.at[index]).wait()


def gather(x, tp, dp, ident):
    return pl.pallas_call(
        functools.partial(gather_kernel, tp, dp),
        out_shape=jax.ShapeDtypeStruct((tp,) + x.shape, x.dtype),
        in_specs=[ANY],
        out_specs=ANY,
        scratch_shapes=[pltpu.SemaphoreType.DMA((tp,)), pltpu.SemaphoreType.DMA((tp,))],
        compiler_params=pltpu.CompilerParams(collective_id=ident, has_side_effects=True),
        name=f"gather_{ident}",
    )(x)


def state_kernel(many, u_ref, are_ref, aim_ref, bre_ref, bim_ref, rre_ref, rim_ref, sre_ref, sim_ref, *rest):
    nre_ref, nim_ref, y_ref = rest[-3:]
    block, channels = u_ref.shape[0], u_ref.shape[1]
    states = are_ref.shape[1]
    cut = 4

    def body(step, carry):
        first = step * many
        for p in range(0, states, 8):
            rows = slice(p, p + 8)
            a_re, a_im = are_ref[0, rows, :], aim_ref[0, rows, :]
            new_re, new_im = [], []
            for b in range(many):
                o_re, o_im = sre_ref[0, first + b, rows, :], sim_ref[0, first + b, rows, :]
                new_re.append(a_re * o_re - a_im * o_im)
                new_im.append(a_re * o_im + a_im * o_re)
            for c in range(channels):
                b_re, b_im = bre_ref[0, c, rows, :], bim_ref[0, c, rows, :]
                for b in range(many):
                    u = u_ref[first + b, c : c + 1, :]
                    new_re[b] = new_re[b] + b_re * u
                    new_im[b] = new_im[b] + b_im * u
            for b in range(many):
                nre_ref[0, first + b, rows, :] = new_re[b]
                nim_ref[0, first + b, rows, :] = new_im[b]
        for c in range(0, channels, cut):
            total = [[None] * many for _ in range(cut)]
            for p in range(0, states, 8):
                rows = slice(p, p + 8)
                h_re = [nre_ref[0, first + b, rows, :] for b in range(many)]
                h_im = [nim_ref[0, first + b, rows, :] for b in range(many)]
                for j in range(cut):
                    r_re, r_im = rre_ref[0, c + j, rows, :], rim_ref[0, c + j, rows, :]
                    for b in range(many):
                        term = r_re * h_re[b] - r_im * h_im[b]
                        total[j][b] = term if p == 0 else total[j][b] + term
            for j in range(cut):
                for b in range(many):
                    y_ref[first + b, c + j : c + j + 1, :] = jnp.sum(
                        total[j][b], axis=0, keepdims=True
                    )
        return carry

    lax.fori_loop(0, block // many, body, 0)


def state_step(layer, u, a_re, a_im, b_re, b_im, r_re, r_im, s_re, s_im, earlier):
    batch, channels, groups = u.shape
    states = a_re.shape[1]
    block = 8
    per_batch = pl.BlockSpec((block, channels, groups), lambda i: (i, 0, 0))
    eigen = pl.BlockSpec((1, states, groups), lambda i: (layer, 0, 0))
    matrix = pl.BlockSpec((1, channels, states, groups), lambda i: (layer, 0, 0, 0))
    state = pl.BlockSpec((1, block, states, groups), lambda i: (layer, i, 0, 0))
    specs = [per_batch, eigen, eigen, matrix, matrix, matrix, matrix, state, state]
    aliases = {}
    if earlier:
        aliases = {len(specs): 0, len(specs) + 1: 1}
    return pl.pallas_call(
        functools.partial(state_kernel, 4),
        grid=(batch // block,),
        out_shape=[
            jax.ShapeDtypeStruct(s_re.shape, jnp.float32),
            jax.ShapeDtypeStruct(s_im.shape, jnp.float32),
            jax.ShapeDtypeStruct(u.shape, jnp.float32),
        ],
        in_specs=specs + [ANY] * len(earlier),
        out_specs=[state, state, per_batch],
        input_output_aliases=aliases,
        name=f"state_{layer}",
    )(u, a_re, a_im, b_re, b_im, r_re, r_im, s_re, s_im, *earlier)


def remote(src, dst, send, recv, target):
    return pltpu.make_async_remote_copy(
        src_ref=src,
        dst_ref=dst,
        send_sem=send,
        recv_sem=recv,
        device_id=target,
        device_id_type=MESH,
    )


def greet(barrier, target):
    pl.semaphore_signal(barrier, inc=1, device_id=target, device_id_type=MESH)


def project_kernel(
    layer, tp, dp, features,
    x_ref, gain_ref, win_ref, wgate_ref, drive_ref, gate_ref,
    xg, wbuf, scaled, acc, squares,
    out1, in1, out2, in2, sq_out1, sq_in1, sq_out2, sq_in2,
    wsem, gsend, grecv, ysend, yrecv, send1, recv1, send2, recv2,
):
    q = tp // dp
    half = dp // 2
    t, d = lax.axis_index("tp"), lax.axis_index("dp")
    z, y = t // q, t % q
    x, c = d // 2, d % 2
    home = z == d
    batch, width = x_ref.shape
    channels = drive_ref.shape[1]
    partner = 2 * x + 1 - c
    far = (d + 2) % dp
    beside = 2 * (far // 2) + 1 - far % 2
    other = 1 - y

    weights = []
    for m, w in enumerate((win_ref, wgate_ref)):
        for h in range(q):
            copy = pltpu.make_async_copy(
                w.at[layer, pl.ds(h * width, width), :], wbuf.at[m, h], wsem.at[m, h]
            )
            copy.start()

    barrier = pltpu.get_barrier_semaphore()
    for e in range(dp):
        @pl.when(jnp.logical_not(jnp.logical_and(home, d == e)))
        def _():
            greet(barrier, {"tp": d * q + y, "dp": e})
    greet(barrier, {"tp": z * q + other})
    greet(barrier, {"dp": partner})
    greet(barrier, {"dp": far})
    pl.semaphore_wait(barrier, dp + 3 - home.astype(jnp.int32))

    upper = z // half
    order = [
        (dp - 1) * (1 - upper),
        half - upper,
        z + 1 - 2 * (z % 2),
        z,
    ]

    def spread(i):
        return remote(
            x_ref, xg.at[y, d], gsend.at[i], grecv.at[d], {"tp": order[i] * q + y, "dp": z}
        )

    for i in range(dp - 1):
        spread(i).start()

    @pl.when(home)
    def _():
        xg[y, d] = x_ref[...]

    @pl.when(jnp.logical_not(home))
    def _():
        spread(dp - 1).start()

    def across(src, e, slot):
        return remote(
            src, xg.at[slot, e], ysend.at[e], yrecv.at[e], {"tp": z * q + other}
        )

    slots = [d, partner, far, beside]
    for i in range(dp):
        e = slots[i]
        if i == 0:
            @pl.when(home)
            def _():
                across(x_ref, e, y).start()

            @pl.when(jnp.logical_not(home))
            def _():
                remote(x_ref, xg.at[y, e], gsend.at[0], grecv.at[e], {"dp": partner}).wait_recv()
                across(xg.at[y, e], e, y).start()
        else:
            remote(x_ref, xg.at[y, e], gsend.at[0], grecv.at[e], {"dp": partner}).wait_recv()
            across(xg.at[y, e], e, y).start()

    def scale(h, first):
        gain = gain_ref[h]
        for e in range(dp):
            xf = xg[h, e].astype(jnp.float32)
            total = jnp.broadcast_to(jnp.sum(xf * xf, axis=1, keepdims=True), squares.shape[1:])
            squares[e] = total if first else squares[e] + total
            scaled[e * batch : (e + 1) * batch, :] = (xf * gain).astype(jnp.bfloat16)

    cut = 256

    scale(y, True)
    for m in range(2):
        pltpu.make_async_copy(
            win_ref.at[layer, pl.ds(0, width), :], wbuf.at[m, y], wsem.at[m, y]
        ).wait()

        def first(n, carry):
            cols = pl.ds(pl.multiple_of(n * cut, cut), cut)
            part = jnp.dot(scaled[...], wbuf[m, y, :, cols], preferred_element_type=jnp.float32)
            acc[m, :, :, cols] = part.reshape(dp, batch, cut)
            return carry

        lax.fori_loop(0, channels // cut, first, 0)

    for i in range(dp):
        e = slots[i]
        across(x_ref, e, other).wait_recv()
    scale(other, False)
    for h in range(half):
        sq_out1[h] = squares[2 * h + 1 - c]
    remote(sq_out1, sq_in1, send1.at[2], recv1.at[2], {"dp": partner}).start()

    def stage1(m):
        return remote(out1.at[m], in1.at[m], send1.at[m], recv1.at[m], {"dp": partner})

    def stage2(m):
        return remote(out2.at[m], in2.at[m], send2.at[m], recv2.at[m], {"dp": far})

    for m in range(2):
        pltpu.make_async_copy(
            win_ref.at[layer, pl.ds(0, width), :], wbuf.at[m, other], wsem.at[m, other]
        ).wait()

        def second(n, carry):
            cols = pl.ds(pl.multiple_of(n * cut, cut), cut)
            part = jnp.dot(
                scaled[...], wbuf[m, other, :, cols], preferred_element_type=jnp.float32
            )
            acc[m, :, :, cols] = acc[m, :, :, cols] + part.reshape(dp, batch, cut)
            for h in range(half):
                out1[m, h, :, cols] = acc[m, 2 * h + 1 - c, :, cols].astype(jnp.bfloat16)
            return carry

        lax.fori_loop(0, channels // cut, second, 0)
        stage1(m).start()

    remote(sq_out1, sq_in1, send1.at[2], recv1.at[2], {"dp": partner}).wait()
    sq_out2[...] = squares[far] + sq_in1[1 - x]
    sq2 = remote(sq_out2, sq_in2, send2.at[2], recv2.at[2], {"dp": far})
    sq2.start()
    for m in range(2):
        stage1(m).wait()
        out2[m] = (acc[m, far] + in1[m, 1 - x].astype(jnp.float32)).astype(jnp.bfloat16)
        stage2(m).start()
        acc[m, d] = acc[m, d] + in1[m, x].astype(jnp.float32)
    sq2.wait()
    meansq = (squares[d] + sq_in1[x] + sq_in2[...])[:, :1] / features
    inverse = lax.rsqrt(meansq + 1e-06)
    for m, result in enumerate((drive_ref, gate_ref)):
        stage2(m).wait()
        result[...] = (acc[m, d] + in2[m].astype(jnp.float32)) * inverse

    for i in range(dp - 1):
        spread(i).wait_send()

    @pl.when(jnp.logical_not(home))
    def _():
        spread(dp - 1).wait_send()

    for i in range(dp):
        across(x_ref, slots[i], y).wait_send()


def project(layer, x, gain, w_input, w_gating, tp, dp, features, ident):
    batch, width = x.shape
    channels = w_input.shape[2]
    q = tp // dp
    half = dp // 2
    bf, f32 = jnp.bfloat16, jnp.float32
    vmem = pl.BlockSpec(memory_space=pltpu.VMEM)
    dma = pltpu.SemaphoreType.DMA
    return pl.pallas_call(
        functools.partial(project_kernel, layer, tp, dp, features),
        out_shape=[jax.ShapeDtypeStruct((batch, channels), f32)] * 2,
        in_specs=[vmem, vmem, ANY, ANY],
        out_specs=[vmem, vmem],
        scratch_shapes=[
            pltpu.VMEM((q, dp, batch, width), bf),
            pltpu.VMEM((2, q, width, channels), bf),
            pltpu.VMEM((dp * batch, width), bf),
            pltpu.VMEM((2, dp, batch, channels), f32),
            pltpu.VMEM((dp, batch, 128), f32),
            pltpu.VMEM((2, half, batch, channels), bf),
            pltpu.VMEM((2, half, batch, channels), bf),
            pltpu.VMEM((2, batch, channels), bf),
            pltpu.VMEM((2, batch, channels), bf),
            pltpu.VMEM((half, batch, 128), f32),
            pltpu.VMEM((half, batch, 128), f32),
            pltpu.VMEM((batch, 128), f32),
            pltpu.VMEM((batch, 128), f32),
            dma((2, q)),
            dma((dp,)),
            dma((dp,)),
            dma((dp,)),
            dma((dp,)),
            dma((3,)),
            dma((3,)),
            dma((3,)),
            dma((3,)),
        ],
        compiler_params=pltpu.CompilerParams(
            collective_id=ident, has_side_effects=True, vmem_limit_bytes=62 * 2**20
        ),
        name=f"project_{layer}",
    )(x, gain, w_input, w_gating)


def merge_kernel(
    layer, tp, dp,
    z_ref, x_ref, w_ref, out_ref,
    both, wbuf, prod, blocks, ybuf, yin, zbuf, zin, own, last, last_in,
    wsem, psend, precv, ysend, yrecv, zsend, zrecv, fsend, frecv,
):
    q = tp // dp
    half = dp // 2
    t, d = lax.axis_index("tp"), lax.axis_index("dp")
    z, y = t // q, t % q
    x, c = d // 2, d % 2
    partner = 2 * x + 1 - c
    other = 1 - y
    batch, width = x_ref.shape
    columns = wbuf.shape[1]
    pieces = 3
    piece = columns // pieces
    collects = z // half == c

    def fetch(n):
        return pltpu.make_async_copy(
            w_ref.at[layer, :, pl.ds(pl.multiple_of(c * columns + n * piece, 128), piece)],
            wbuf.at[:, pl.ds(n * piece, piece)],
            wsem.at[n],
        )

    for n in range(pieces):
        fetch(n).start()

    barrier = pltpu.get_barrier_semaphore()
    greet(barrier, {"dp": partner})
    greet(barrier, {"tp": z * q + other})

    @pl.when(collects)
    def _():
        for o in range(1, dp):
            greet(barrier, {"tp": ((z + o) % dp) * q + y})

    pl.semaphore_wait(barrier, 2 + half - collects.astype(jnp.int32))

    swap = remote(z_ref, both.at[c], psend, precv, {"dp": partner})
    swap.start()
    both[c] = z_ref[...]
    remote(z_ref, both.at[1 - c], psend, precv, {"dp": partner}).wait_recv()
    rows = both[...].reshape(2 * batch, both.shape[2])
    for n in range(pieces):
        fetch(n).wait()
        span = slice(n * piece, (n + 1) * piece)
        prod[:, span] = jnp.dot(rows, wbuf[:, span], preferred_element_type=jnp.float32)
    for j in range(half * q):
        for e in range(2):
            blocks[j, e] = prod[e * batch : (e + 1) * batch, j * width : (j + 1) * width]

    first = jnp.where(c == 0, jnp.where(z == 0, 1, 0), jnp.where(z == dp - 1, 0, 1))
    turns = [first, 1 - first]

    def over_y(k, e):
        return remote(
            ybuf.at[k, e], yin.at[k, e], ysend.at[k, e], yrecv.at[k, e], {"tp": z * q + other}
        )

    def over_z(k, e):
        return remote(
            zbuf.at[k, e],
            zin.at[z, e],
            zsend.at[k, e],
            zrecv.at[z, e],
            {"tp": (half * c + k) * q + y},
        )

    for k in turns:
        for e in range(2):
            ybuf[k, e] = blocks[q * k + other, e].astype(jnp.bfloat16)
            over_y(k, e).start()
    for k in turns:
        mine = half * c + k == z
        for e in range(2):
            over_y(k, e).wait_recv()
            total = blocks[q * k + y, e] + yin[k, e].astype(jnp.float32)

            @pl.when(mine)
            def _():
                own[e] = total

            @pl.when(jnp.logical_not(mine))
            def _():
                zbuf[k, e] = total.astype(jnp.bfloat16)
                over_z(k, e).start()

    final = remote(last, last_in, fsend, frecv, {"dp": partner})

    def gathered(e):
        total = own[e]
        for o in range(1, dp):
            source = (z + o) % dp
            remote(
                zbuf.at[0, 0], zin.at[source, e], zsend.at[0, 0], zrecv.at[source, e],
                {"dp": partner},
            ).wait_recv()
            total = total + zin[source, e].astype(jnp.float32)
        return total

    @pl.when(collects)
    def _():
        last[...] = gathered(1 - c)
        final.start()
        out_ref[...] = (x_ref[...].astype(jnp.float32) + gathered(c)).astype(jnp.bfloat16)
        final.wait_send()

    @pl.when(jnp.logical_not(collects))
    def _():
        final.wait_recv()
        out_ref[...] = (x_ref[...].astype(jnp.float32) + last_in[...]).astype(jnp.bfloat16)

    swap.wait_send()
    for k in range(2):
        for e in range(2):
            over_y(k, e).wait_send()

            @pl.when(half * c + k != z)
            def _():
                over_z(k, e).wait_send()


def merge(layer, gated, x, w_output, tp, dp, ident):
    batch, width = x.shape
    channels, features = w_output.shape[1:]
    q = tp // dp
    half = dp // 2
    bf, f32 = jnp.bfloat16, jnp.float32
    vmem = pl.BlockSpec(memory_space=pltpu.VMEM)
    dma = pltpu.SemaphoreType.DMA
    return pl.pallas_call(
        functools.partial(merge_kernel, layer, tp, dp),
        out_shape=jax.ShapeDtypeStruct((batch, width), bf),
        in_specs=[vmem, vmem, ANY],
        out_specs=vmem,
        scratch_shapes=[
            pltpu.VMEM((2, batch, channels), bf),
            pltpu.VMEM((channels, features // 2), bf),
            pltpu.VMEM((2 * batch, features // 2), f32),
            pltpu.VMEM((half * q, 2, batch, width), f32),
            pltpu.VMEM((half, 2, batch, width), bf),
            pltpu.VMEM((half, 2, batch, width), bf),
            pltpu.VMEM((half, 2, batch, width), bf),
            pltpu.VMEM((dp, 2, batch, width), bf),
            pltpu.VMEM((2, batch, width), f32),
            pltpu.VMEM((batch, width), f32),
            pltpu.VMEM((batch, width), f32),
            dma((3,)),
            dma,
            dma,
            dma((half, 2)),
            dma((half, 2)),
            dma((half, 2)),
            dma((dp, 2)),
            dma,
            dma,
        ],
        compiler_params=pltpu.CompilerParams(
            collective_id=ident, has_side_effects=True, vmem_limit_bytes=62 * 2**20
        ),
        name=f"merge_{layer}",
    )(gated, x, w_output)


def on_device(
    tp,
    dp,
    tokens,
    gains,
    w_input,
    w_gating,
    w_output,
    decay_rate,
    frequency,
    log_step,
    in_real,
    in_imag,
    readout_real_matrix,
    readout_imag_matrix,
    skip_gain,
    state_real,
    state_imag,
):
    batch, width = tokens.shape
    groups, states = decay_rate.shape[1:]
    channels = groups * GS
    rows = w_input.shape[1]
    features = gains.shape[1]
    q = tp // dp
    d = lax.axis_index("dp")

    step = jnp.exp(log_step)[:, None, :]
    lam_re = -jnp.swapaxes(decay_rate, 1, 2)
    lam_im = jnp.swapaxes(frequency, 1, 2)
    magnitude = jnp.exp(lam_re * step)
    angle = lam_im * step
    abar_re = magnitude * jnp.cos(angle)
    abar_im = magnitude * jnp.sin(angle)
    denom = lam_re * lam_re + lam_im * lam_im
    num_re = abar_re - 1.0
    zoh_re = ((num_re * lam_re + abar_im * lam_im) / denom)[:, None]
    zoh_im = ((abar_im * lam_re - num_re * lam_im) / denom)[:, None]
    i_re = jnp.transpose(in_real, (0, 3, 2, 1))
    i_im = jnp.transpose(in_imag, (0, 3, 2, 1))
    bbar_re = zoh_re * i_re - zoh_im * i_im
    bbar_im = zoh_re * i_im + zoh_im * i_re
    r_re = jnp.transpose(readout_real_matrix, (0, 2, 3, 1))
    r_im = jnp.transpose(readout_imag_matrix, (0, 2, 3, 1))
    s_re = jnp.swapaxes(state_real, 2, 3)
    s_im = jnp.swapaxes(state_imag, 2, 3)
    my_gains = lax.dynamic_slice_in_dim(gains, d * rows, rows, 1).reshape(LAYERS, q, 1, width)

    shard = tokens
    news = ()
    paired = q == 2 and dp == 4
    for layer in range(LAYERS):
        if paired:
            drive, gate = project(
                layer, shard, my_gains[layer], w_input, w_gating, tp, dp, features, 2 * layer + 1
            )
            u = jnp.swapaxes(drive.reshape(batch, groups, GS), 1, 2)
            n_re, n_im, y = state_step(
                layer, u, abar_re, abar_im, bbar_re, bbar_im, r_re, r_im, s_re, s_im, news
            )
            news = (n_re, n_im)
            y = jnp.swapaxes(y, 1, 2).reshape(batch, channels) + skip_gain[layer][None] * drive
            z = (jax.nn.gelu(y) * jax.nn.sigmoid(gate)).astype(jnp.bfloat16)
            shard = merge(layer, z, shard, w_output, tp, dp, 2 * layer + 2)
            continue
        got = gather(shard, tp, dp, 3 * layer + 1).reshape(q, dp * batch, width)
        xf = got.astype(jnp.float32)
        squares = jnp.sum(xf * xf, axis=(0, 2))
        scaled = (xf * my_gains[layer]).astype(jnp.bfloat16)
        if q <= 2:
            scaled = jnp.concatenate([scaled[h] for h in range(q)], axis=1)
        else:
            scaled = jnp.swapaxes(scaled, 0, 1).reshape(dp * batch, rows)
        drive = jnp.dot(scaled, w_input[layer], preferred_element_type=jnp.float32)
        gate = jnp.dot(scaled, w_gating[layer], preferred_element_type=jnp.float32)
        drive, gate, squares = exchange(
            [
                drive.astype(jnp.bfloat16).reshape(dp, batch, channels),
                gate.astype(jnp.bfloat16).reshape(dp, batch, channels),
                jnp.broadcast_to(squares.reshape(dp, batch, 1), (dp, batch, 128)),
            ],
            "dp",
            dp,
            3 * layer + 2,
        )
        meansq = jnp.sum(squares, axis=0)[:, :1] / features
        inverse = lax.rsqrt(meansq + 1e-06)
        drive = jnp.sum(drive.astype(jnp.float32), axis=0) * inverse
        gate = jnp.sum(gate.astype(jnp.float32), axis=0) * inverse
        u = jnp.swapaxes(drive.reshape(batch, groups, GS), 1, 2)
        n_re, n_im, y = state_step(
            layer, u, abar_re, abar_im, bbar_re, bbar_im, r_re, r_im, s_re, s_im, news
        )
        news = (n_re, n_im)
        y = jnp.swapaxes(y, 1, 2).reshape(batch, channels) + skip_gain[layer][None] * drive
        z = (jax.nn.gelu(y) * jax.nn.sigmoid(gate)).astype(jnp.bfloat16)
        branch = jnp.dot(z, w_output[layer], preferred_element_type=jnp.float32)
        pieces = jnp.swapaxes(branch.astype(jnp.bfloat16).reshape(batch, tp, width), 0, 1)
        (pieces,) = exchange([pieces], "tp", tp, 3 * layer + 3)
        summed = jnp.sum(pieces.astype(jnp.float32), axis=0)
        shard = (shard.astype(jnp.float32) + summed).astype(jnp.bfloat16)
    return shard, jnp.swapaxes(news[0], 2, 3), jnp.swapaxes(news[1], 2, 3)


def solution(mesh):
    placed = (
        P("dp", "tp"),
        P(),
        P(None, "dp", "tp"),
        P(None, "dp", "tp"),
        P(None, "tp", None),
        P(None, "tp", None),
        P(None, "tp", None),
        P(None, "tp"),
        P(None, "tp", None, None),
        P(None, "tp", None, None),
        P(None, "tp", None, None),
        P(None, "tp", None, None),
        P(None, "tp"),
        P(None, "dp", "tp", None),
        P(None, "dp", "tp", None),
    )
    return jax.shard_map(
        functools.partial(on_device, mesh.shape["tp"], mesh.shape["dp"]),
        mesh=mesh,
        in_specs=placed,
        out_specs=(P("dp", "tp"), P(None, "dp", "tp", None), P(None, "dp", "tp", None)),
        check_vma=False,
    )
```

```python
import functools

import jax
import jax.numpy as jnp
from jax import lax
from jax.experimental import pallas as pl
from jax.experimental.pallas import tpu as pltpu
from jax.sharding import PartitionSpec as P

GS = 16
LAYERS = 2
MESH = pl.DeviceIdType.MESH
ANY = pl.BlockSpec(memory_space=pl.ANY)


def exchange_kernel(axis, n, count, *refs):
    ins, outs = refs[:count], refs[count : 2 * count]
    send, recv, local = refs[2 * count :]
    me = lax.axis_index(axis)
    barrier = pltpu.get_barrier_semaphore()
    for i in range(1, n):
        pl.semaphore_signal(
            barrier, inc=1, device_id={axis: lax.rem(me + i, n)}, device_id_type=MESH
        )
    own = [
        pltpu.make_async_copy(ins[k].at[me], outs[k].at[me], local.at[k]) for k in range(count)
    ]
    for copy in own:
        copy.start()
    pl.semaphore_wait(barrier, n - 1)
    copies = []
    for i in range(1, n):
        peer = lax.rem(me + i, n)
        for k in range(count):
            copy = pltpu.make_async_remote_copy(
                src_ref=ins[k].at[peer],
                dst_ref=outs[k].at[me],
                send_sem=send.at[k, i],
                recv_sem=recv.at[k, i],
                device_id={axis: peer},
                device_id_type=MESH,
            )
            copy.start()
            copies.append((i, k, copy))
    for copy in own:
        copy.wait()
    for i, k, copy in copies:
        copy.wait_send()
        source = lax.rem(me + n - i, n)
        pltpu.make_async_remote_copy(
            src_ref=ins[k].at[source],
            dst_ref=outs[k].at[source],
            send_sem=send.at[k, i],
            recv_sem=recv.at[k, i],
            device_id={axis: source},
            device_id_type=MESH,
        ).wait_recv()


def exchange(arrays, axis, n, ident):
    count = len(arrays)
    return pl.pallas_call(
        functools.partial(exchange_kernel, axis, n, count),
        out_shape=[jax.ShapeDtypeStruct(a.shape, a.dtype) for a in arrays],
        in_specs=[ANY] * count,
        out_specs=[ANY] * count,
        scratch_shapes=[
            pltpu.SemaphoreType.DMA((count, n)),
            pltpu.SemaphoreType.DMA((count, n)),
            pltpu.SemaphoreType.DMA((count,)),
        ],
        compiler_params=pltpu.CompilerParams(collective_id=ident, has_side_effects=True),
        name=f"exchange_{axis}_{ident}",
    )(*arrays)


def gather_kernel(tp, dp, x_ref, out_ref, send, recv):
    q = tp // dp
    t = lax.axis_index("tp")
    d = lax.axis_index("dp")
    group = t // q
    slot = lax.rem(t, q) * dp + d
    barrier = pltpu.get_barrier_semaphore()
    for h in range(q):
        for r in range(dp):
            source = d * q + h
            pl.semaphore_signal(
                barrier, inc=1, device_id={"tp": source, "dp": r}, device_id_type=MESH
            )

    pl.semaphore_wait(barrier, tp)

    def remote(i, index):
        return pltpu.make_async_remote_copy(
            src_ref=x_ref,
            dst_ref=out_ref.at[index],
            send_sem=send.at[i],
            recv_sem=recv.at[index],
            device_id={"tp": lax.rem(t + i, tp), "dp": group},
            device_id_type=MESH,
        )

    home = group == d

    @pl.when(home)
    def _():
        pltpu.make_async_copy(x_ref, out_ref.at[slot], recv.at[slot]).start()

    @pl.when(jnp.logical_not(home))
    def _():
        remote(0, slot).start()

    for i in range(1, tp):
        remote(i, slot).start()
    for i in range(1, tp):
        remote(i, slot).wait_send()

    @pl.when(jnp.logical_not(home))
    def _():
        remote(0, slot).wait_send()

    for index in range(tp):
        pltpu.make_async_copy(x_ref, out_ref.at[index], recv.at[index]).wait()


def gather(x, tp, dp, ident):
    return pl.pallas_call(
        functools.partial(gather_kernel, tp, dp),
        out_shape=jax.ShapeDtypeStruct((tp,) + x.shape, x.dtype),
        in_specs=[ANY],
        out_specs=ANY,
        scratch_shapes=[pltpu.SemaphoreType.DMA((tp,)), pltpu.SemaphoreType.DMA((tp,))],
        compiler_params=pltpu.CompilerParams(collective_id=ident, has_side_effects=True),
        name=f"gather_{ident}",
    )(x)


def state_kernel(many, u_ref, are_ref, aim_ref, bre_ref, bim_ref, rre_ref, rim_ref, sre_ref, sim_ref, *rest):
    nre_ref, nim_ref, y_ref = rest[-3:]
    block, channels = u_ref.shape[0], u_ref.shape[1]
    states = are_ref.shape[1]
    cut = 4

    def body(step, carry):
        first = step * many
        for p in range(0, states, 8):
            rows = slice(p, p + 8)
            a_re, a_im = are_ref[0, rows, :], aim_ref[0, rows, :]
            new_re, new_im = [], []
            for b in range(many):
                o_re, o_im = sre_ref[0, first + b, rows, :], sim_ref[0, first + b, rows, :]
                new_re.append(a_re * o_re - a_im * o_im)
                new_im.append(a_re * o_im + a_im * o_re)
            for c in range(channels):
                b_re, b_im = bre_ref[0, c, rows, :], bim_ref[0, c, rows, :]
                for b in range(many):
                    u = u_ref[first + b, c : c + 1, :]
                    new_re[b] = new_re[b] + b_re * u
                    new_im[b] = new_im[b] + b_im * u
            for b in range(many):
                nre_ref[0, first + b, rows, :] = new_re[b]
                nim_ref[0, first + b, rows, :] = new_im[b]
        for c in range(0, channels, cut):
            total = [[None] * many for _ in range(cut)]
            for p in range(0, states, 8):
                rows = slice(p, p + 8)
                h_re = [nre_ref[0, first + b, rows, :] for b in range(many)]
                h_im = [nim_ref[0, first + b, rows, :] for b in range(many)]
                for j in range(cut):
                    r_re, r_im = rre_ref[0, c + j, rows, :], rim_ref[0, c + j, rows, :]
                    for b in range(many):
                        term = r_re * h_re[b] - r_im * h_im[b]
                        total[j][b] = term if p == 0 else total[j][b] + term
            for j in range(cut):
                for b in range(many):
                    y_ref[first + b, c + j : c + j + 1, :] = jnp.sum(
                        total[j][b], axis=0, keepdims=True
                    )
        return carry

    lax.fori_loop(0, block // many, body, 0)


def state_step(layer, u, a_re, a_im, b_re, b_im, r_re, r_im, s_re, s_im, earlier):
    batch, channels, groups = u.shape
    states = a_re.shape[1]
    block = 8
    per_batch = pl.BlockSpec((block, channels, groups), lambda i: (i, 0, 0))
    eigen = pl.BlockSpec((1, states, groups), lambda i: (layer, 0, 0))
    matrix = pl.BlockSpec((1, channels, states, groups), lambda i: (layer, 0, 0, 0))
    state = pl.BlockSpec((1, block, states, groups), lambda i: (layer, i, 0, 0))
    specs = [per_batch, eigen, eigen, matrix, matrix, matrix, matrix, state, state]
    aliases = {}
    if earlier:
        aliases = {len(specs): 0, len(specs) + 1: 1}
    return pl.pallas_call(
        functools.partial(state_kernel, 4),
        grid=(batch // block,),
        out_shape=[
            jax.ShapeDtypeStruct(s_re.shape, jnp.float32),
            jax.ShapeDtypeStruct(s_im.shape, jnp.float32),
            jax.ShapeDtypeStruct(u.shape, jnp.float32),
        ],
        in_specs=specs + [ANY] * len(earlier),
        out_specs=[state, state, per_batch],
        input_output_aliases=aliases,
        name=f"state_{layer}",
    )(u, a_re, a_im, b_re, b_im, r_re, r_im, s_re, s_im, *earlier)


def remote(src, dst, send, recv, target):
    return pltpu.make_async_remote_copy(
        src_ref=src,
        dst_ref=dst,
        send_sem=send,
        recv_sem=recv,
        device_id=target,
        device_id_type=MESH,
    )


def greet(barrier, target):
    pl.semaphore_signal(barrier, inc=1, device_id=target, device_id_type=MESH)


def layer_kernel(
    layer, tp, dp, features, earlier,
    x_ref, gain_ref, skip_ref, win_ref, wgate_ref, wout_ref,
    logstep_ref, decay_ref, freq_ref, ire_ref, iim_ref, rre_ref, rim_ref, sre_ref, sim_ref,
    *rest,
):
    out_ref, nre_ref, nim_ref = rest[earlier : earlier + 3]
    (
        xg, wbuf, scaled, acc, squares,
        out1, in1, out2, in2, sq_out1, sq_in1, sq_out2, sq_in2,
        decay, freq, i_re, i_im,
        a_re, a_im, b_re, b_im, r_re, r_im, h_re, h_im,
        mix, y0, y0p, y3, u3, ub, flip, flipy, unat, gated,
        both, wobuf, prod, blocks, ybuf, yin, zbuf, zin, own, last, last_in,
        wsem, gsend, grecv, across_send, across_recv, send1, recv1, send2, recv2,
        ssem, osem, psem, swap_send, swap_recv, ysend, yrecv, zsend, zrecv, fsend, frecv,
    ) = rest[earlier + 3 :]
    q = tp // dp
    half = dp // 2
    t, d = lax.axis_index("tp"), lax.axis_index("dp")
    z, y = t // q, t % q
    x, c = d // 2, d % 2
    home = z == d
    batch, width = x_ref.shape
    channels = unat.shape[1]
    states, groups = a_re.shape
    gs = channels // groups
    partner = 2 * x + 1 - c
    far = (d + 2) % dp
    beside = 2 * (far // 2) + 1 - far % 2
    other = 1 - y
    collects = z // half == c
    columns = wobuf.shape[1]
    pieces = 3
    piece = columns // pieces

    params = [
        pltpu.make_async_copy(src.at[layer], dst, ssem.at[i])
        for i, (src, dst) in enumerate(
            (
                (decay_ref, decay), (freq_ref, freq), (ire_ref, i_re), (iim_ref, i_im),
                (rre_ref, r_re), (rim_ref, r_im), (sre_ref, h_re), (sim_ref, h_im),
            )
        )
    ]
    for copy in params:
        copy.start()
    def fetch(n):
        return pltpu.make_async_copy(
            wout_ref.at[layer, :, pl.ds(pl.multiple_of(c * columns + n * piece, 128), piece)],
            wobuf.at[:, pl.ds(n * piece, piece)],
            osem.at[n],
        )

    barrier = pltpu.get_barrier_semaphore()
    for e in range(dp):
        @pl.when(jnp.logical_not(jnp.logical_and(home, d == e)))
        def _():
            greet(barrier, {"tp": d * q + y, "dp": e})
    greet(barrier, {"tp": z * q + other})
    greet(barrier, {"dp": partner})
    greet(barrier, {"dp": far})

    @pl.when(collects)
    def _():
        for o in range(1, dp):
            greet(barrier, {"tp": ((z + o) % dp) * q + y})

    pl.semaphore_wait(
        barrier, dp + 3 + half - home.astype(jnp.int32) - collects.astype(jnp.int32)
    )

    upper = z // half
    order = [
        (dp - 1) * (1 - upper),
        half - upper,
        z + 1 - 2 * (z % 2),
        z,
    ]

    def spread(i):
        return remote(
            x_ref, xg.at[y, d], gsend.at[i], grecv.at[d], {"tp": order[i] * q + y, "dp": z}
        )

    for i in range(dp - 1):
        spread(i).start()

    @pl.when(home)
    def _():
        xg[y, d] = x_ref[...]

    @pl.when(jnp.logical_not(home))
    def _():
        spread(dp - 1).start()

    def across(src, e, slot):
        return remote(
            src, xg.at[slot, e], across_send.at[e], across_recv.at[e], {"tp": z * q + other}
        )

    slots = [d, partner, far, beside]
    many, cut = 4, 4

    def mixing(o, carry):
        for i in range(0, gs, cut):
            total = [None] * cut
            for p in range(0, states, 8):
                rows = slice(p, p + 8)
                left_re, left_im = r_re[o, rows, :], r_im[o, rows, :]
                for j in range(cut):
                    term = left_re * b_re[i + j, rows, :] - left_im * b_im[i + j, rows, :]
                    total[j] = term if p == 0 else total[j] + term
            for j in range(cut):
                mix[o, i + j : i + j + 1, :] = jnp.sum(total[j], axis=0, keepdims=True)
        return carry

    def recall(step, carry):
        first = step * many
        for p in range(0, states, 8):
            rows = slice(p, p + 8)
            pole_re, pole_im = a_re[rows, :], a_im[rows, :]
            for b in range(many):
                o_re, o_im = h_re[first + b, rows, :], h_im[first + b, rows, :]
                h_re[first + b, rows, :] = pole_re * o_re - pole_im * o_im
                h_im[first + b, rows, :] = pole_re * o_im + pole_im * o_re
        for i in range(0, gs, cut):
            total = [[None] * many for _ in range(cut)]
            for p in range(0, states, 8):
                rows = slice(p, p + 8)
                n_re = [h_re[first + b, rows, :] for b in range(many)]
                n_im = [h_im[first + b, rows, :] for b in range(many)]
                for j in range(cut):
                    left_re, left_im = r_re[i + j, rows, :], r_im[i + j, rows, :]
                    for b in range(many):
                        term = left_re * n_re[b] - left_im * n_im[b]
                        total[j][b] = term if p == 0 else total[j][b] + term
            for j in range(cut):
                for b in range(many):
                    y0[first + b, i + j : i + j + 1, :] = jnp.sum(
                        total[j][b], axis=0, keepdims=True
                    )
        return carry

    def push(step, carry):
        first = step * many
        for p in range(0, states, 8):
            rows = slice(p, p + 8)
            n_re = [h_re[first + b, rows, :] for b in range(many)]
            n_im = [h_im[first + b, rows, :] for b in range(many)]
            for i in range(gs):
                in_re, in_im = b_re[i, rows, :], b_im[i, rows, :]
                for b in range(many):
                    u = ub[first + b, i : i + 1, :]
                    n_re[b] = n_re[b] + in_re * u
                    n_im[b] = n_im[b] + in_im * u
            for b in range(many):
                h_re[first + b, rows, :] = n_re[b]
                h_im[first + b, rows, :] = n_im[b]
        return carry

    for copy in params[:4]:
        copy.wait()
    step = jnp.exp(logstep_ref[layer : layer + 1, :])
    lam_re, lam_im = -decay[...], freq[...]
    magnitude = jnp.exp(lam_re * step)
    angle = lam_im * step
    pole_re, pole_im = magnitude * jnp.cos(angle), magnitude * jnp.sin(angle)
    denom = lam_re * lam_re + lam_im * lam_im
    num_re = pole_re - 1.0
    a_re[...] = pole_re
    a_im[...] = pole_im
    zoh_re = (num_re * lam_re + pole_im * lam_im) / denom
    zoh_im = (pole_im * lam_re - num_re * lam_im) / denom
    flat_re, flat_im = i_re.reshape(states * gs, groups), i_im.reshape(states * gs, groups)
    for i in range(gs):
        col = pl.ds(i, states, stride=gs)
        in_re, in_im = flat_re[col, :], flat_im[col, :]
        b_re[i] = zoh_re * in_re - zoh_im * in_im
        b_im[i] = zoh_re * in_im + zoh_im * in_re
    for copy in params[4:]:
        copy.wait()
    for m, w in enumerate((win_ref, wgate_ref)):
        for h in range(q):
            pltpu.make_async_copy(
                w.at[layer, pl.ds(h * width, width), :], wbuf.at[m, h], wsem.at[m, h]
            ).start()
    lax.fori_loop(0, gs, mixing, 0)
    steps = batch // many
    marks = [(i * steps) // dp for i in range(dp + 1)]
    for i in range(dp):
        lax.fori_loop(marks[i], marks[i + 1], recall, 0)
        e = slots[i]
        if i == 0:
            @pl.when(home)
            def _():
                across(x_ref, e, y).start()

            @pl.when(jnp.logical_not(home))
            def _():
                remote(x_ref, xg.at[y, e], gsend.at[0], grecv.at[e], {"dp": partner}).wait_recv()
                across(xg.at[y, e], e, y).start()
        else:
            remote(x_ref, xg.at[y, e], gsend.at[0], grecv.at[e], {"dp": partner}).wait_recv()
            across(xg.at[y, e], e, y).start()

    def scale(h, first):
        gain = gain_ref[layer, pl.ds(d * q + h, 1), :]
        for e in range(dp):
            xf = xg[h, e].astype(jnp.float32)
            total = jnp.broadcast_to(jnp.sum(xf * xf, axis=1, keepdims=True), squares.shape[1:])
            squares[e] = total if first else squares[e] + total
            scaled[e * batch : (e + 1) * batch, :] = (xf * gain).astype(jnp.bfloat16)

    tile = channels // 2

    scale(y, True)
    for m in range(2):
        pltpu.make_async_copy(
            win_ref.at[layer, pl.ds(0, width), :], wbuf.at[m, y], wsem.at[m, y]
        ).wait()

        def first(n, carry):
            cols = pl.ds(pl.multiple_of(n * tile, 128), tile)
            part = jnp.dot(scaled[...], wbuf[m, y, :, cols], preferred_element_type=jnp.float32)
            acc[m, :, :, cols] = part.reshape(dp, batch, tile)
            return carry

        lax.fori_loop(0, channels // tile, first, 0)

    for n in range(pieces):
        fetch(n).start()
    flat = y0.reshape(batch * gs, groups)
    for i in range(gs):
        y0p[i] = flat[pl.ds(i, batch, stride=gs), :]

    for i in range(dp):
        across(x_ref, slots[i], other).wait_recv()
    scale(other, False)
    for h in range(half):
        sq_out1[h] = squares[2 * h + 1 - c]
    sq1 = remote(sq_out1, sq_in1, send1.at[2], recv1.at[2], {"dp": partner})
    sq1.start()

    def stage1(m):
        return remote(out1.at[m], in1.at[m], send1.at[m], recv1.at[m], {"dp": partner})

    def stage2(m):
        return remote(out2.at[m], in2.at[m], send2.at[m], recv2.at[m], {"dp": far})

    for m in range(2):
        pltpu.make_async_copy(
            win_ref.at[layer, pl.ds(0, width), :], wbuf.at[m, other], wsem.at[m, other]
        ).wait()

        def second(n, carry):
            cols = pl.ds(pl.multiple_of(n * tile, 128), tile)
            part = jnp.dot(
                scaled[...], wbuf[m, other, :, cols], preferred_element_type=jnp.float32
            )
            acc[m, :, :, cols] = acc[m, :, :, cols] + part.reshape(dp, batch, tile)
            for h in range(half):
                out1[m, h, :, cols] = acc[m, 2 * h + 1 - c, :, cols].astype(jnp.bfloat16)
            return carry

        lax.fori_loop(0, channels // tile, second, 0)
        stage1(m).start()

    sq1.wait()
    sq_out2[...] = squares[far] + sq_in1[1 - x]
    sq2 = remote(sq_out2, sq_in2, send2.at[2], recv2.at[2], {"dp": far})
    sq2.start()
    for m in range(2):
        stage1(m).wait()
        out2[m] = (acc[m, far] + in1[m, 1 - x].astype(jnp.float32)).astype(jnp.bfloat16)
        stage2(m).start()
        acc[m, d] = acc[m, d] + in1[m, x].astype(jnp.float32)
    sq2.wait()
    meansq = (squares[d] + sq_in1[x] + sq_in2[...])[:, :1] / features
    inverse = lax.rsqrt(meansq + 1e-06)
    stage2(0).wait()
    drive = (acc[0, d] + in2[0].astype(jnp.float32)) * inverse
    unat[...] = drive
    flip[...] = drive.T
    for i in range(gs):
        u3[i] = flip[pl.ds(i, groups, stride=gs), :].T

    def respond(n, carry):
        rows = pl.ds(pl.multiple_of(n * 8, 8), 8)
        u = [u3[i, rows, :] for i in range(gs)]
        for o in range(gs):
            total = y0p[o, rows, :]
            for i in range(gs):
                total = total + mix[o, i : i + 1, :] * u[i]
            y3[o, rows, :] = total
        return carry

    lax.fori_loop(0, batch // 8, respond, 0)
    for i in range(gs):
        flipy[pl.ds(i, groups, stride=gs), :] = y3[i].T
    read = flipy[...].T + skip_ref[layer : layer + 1, :] * unat[...]
    stage2(1).wait()
    gate = (acc[1, d] + in2[1].astype(jnp.float32)) * inverse
    gated[...] = (jax.nn.gelu(read) * jax.nn.sigmoid(gate)).astype(jnp.bfloat16)

    swap = remote(gated, both.at[c], swap_send, swap_recv, {"dp": partner})
    swap.start()
    both[c] = gated[...]
    flat_u = u3.reshape(gs * batch, groups)
    for b in range(batch):
        ub[b] = flat_u[pl.ds(b, gs, stride=batch), :]
    remote(gated, both.at[1 - c], swap_send, swap_recv, {"dp": partner}).wait_recv()
    first_turn = jnp.where(c == 0, jnp.where(z == 0, 1, 0), jnp.where(z == dp - 1, 0, 1))
    turns = [first_turn, 1 - first_turn]

    def over_y(k, e):
        return remote(
            ybuf.at[k, e], yin.at[k, e], ysend.at[k, e], yrecv.at[k, e], {"tp": z * q + other}
        )

    def over_z(k, e):
        return remote(
            zbuf.at[k, e],
            zin.at[z, e],
            zsend.at[k, e],
            zrecv.at[z, e],
            {"tp": (half * c + k) * q + y},
        )

    rows = both[...].reshape(2 * batch, channels)

    def multiply(n):
        pltpu.make_async_copy(
            wout_ref.at[layer, :, pl.ds(0, piece)], wobuf.at[:, pl.ds(0, piece)], osem.at[n]
        ).wait()
        span = pl.ds(pl.multiple_of(n * piece, 128), piece)
        prod[:, span] = jnp.dot(rows, wobuf[:, span], preferred_element_type=jnp.float32)

    def send_over_y(k):
        for static in range(half):
            @pl.when(k == static)
            def _():
                for j in range(static * q, (static + 1) * q):
                    for e in range(2):
                        blocks[j, e] = prod[
                            e * batch : (e + 1) * batch, j * width : (j + 1) * width
                        ]
        for e in range(2):
            ybuf[k, e] = blocks[q * k + other, e].astype(jnp.bfloat16)
            over_y(k, e).start()

    multiply((pieces - 1) * first_turn)
    multiply(1)
    send_over_y(turns[0])
    multiply((pieces - 1) * turns[1])
    send_over_y(turns[1])
    lax.fori_loop(0, steps, push, 0)
    results = [
        pltpu.make_async_copy(h_re, nre_ref.at[layer], psem.at[0]),
        pltpu.make_async_copy(h_im, nim_ref.at[layer], psem.at[1]),
    ]
    for copy in results:
        copy.start()
    for k in turns:
        mine = half * c + k == z
        for e in range(2):
            over_y(k, e).wait_recv()
            total = blocks[q * k + y, e] + yin[k, e].astype(jnp.float32)

            @pl.when(mine)
            def _():
                own[e] = total

            @pl.when(jnp.logical_not(mine))
            def _():
                zbuf[k, e] = total.astype(jnp.bfloat16)
                over_z(k, e).start()

    def finish(total):
        if layer == LAYERS - 1:
            out_ref[...] = total
        else:
            out_ref[...] = (x_ref[...].astype(jnp.float32) + total).astype(jnp.bfloat16)

    final = remote(last, last_in, fsend, frecv, {"dp": partner})

    def gathered(e):
        total = own[e]
        for o in range(1, dp):
            source = (z + o) % dp
            remote(
                zbuf.at[0, 0], zin.at[source, e], zsend.at[0, 0], zrecv.at[source, e],
                {"dp": partner},
            ).wait_recv()
            total = total + zin[source, e].astype(jnp.float32)
        return total

    @pl.when(collects)
    def _():
        last[...] = gathered(1 - c)
        final.start()
        finish(gathered(c))
        final.wait_send()

    @pl.when(jnp.logical_not(collects))
    def _():
        final.wait_recv()
        finish(last_in[...])

    for copy in results:
        copy.wait()
    for i in range(dp - 1):
        spread(i).wait_send()

    @pl.when(jnp.logical_not(home))
    def _():
        spread(dp - 1).wait_send()

    for i in range(dp):
        across(x_ref, slots[i], y).wait_send()
    swap.wait_send()
    for k in range(2):
        for e in range(2):
            over_y(k, e).wait_send()

            @pl.when(half * c + k != z)
            def _():
                over_z(k, e).wait_send()


def layer_step(
    layer, x, gain, skip, w_input, w_gating, w_output, log_step, eigen, state, earlier, tp, dp, ident
):
    batch, width = x.shape
    channels = w_input.shape[2]
    states, groups = eigen[0].shape[1:]
    gs = channels // groups
    features = w_output.shape[2]
    q = tp // dp
    half = dp // 2
    bf, f32 = jnp.bfloat16, jnp.float32
    vmem = pl.BlockSpec(memory_space=pltpu.VMEM)
    dma = pltpu.SemaphoreType.DMA
    operands = [
        x, gain, skip, w_input, w_gating, w_output, log_step, *eigen, *state, *earlier
    ]
    aliases = {len(operands) - 2: 1, len(operands) - 1: 2} if earlier else {}
    return pl.pallas_call(
        functools.partial(layer_kernel, layer, tp, dp, features, len(earlier)),
        out_shape=[jax.ShapeDtypeStruct((batch, width), f32 if layer == LAYERS - 1 else bf)]
        + [jax.ShapeDtypeStruct(a.shape, f32) for a in state],
        in_specs=[vmem] * 3 + [ANY] * 3 + [vmem] + [ANY] * (len(operands) - 7),
        out_specs=[vmem, ANY, ANY],
        input_output_aliases=aliases,
        scratch_shapes=[
            pltpu.VMEM((q, dp, batch, width), bf),
            pltpu.VMEM((2, q, width, channels), bf),
            pltpu.VMEM((dp * batch, width), bf),
            pltpu.VMEM((2, dp, batch, channels), f32),
            pltpu.VMEM((dp, batch, 128), f32),
            pltpu.VMEM((2, half, batch, channels), bf),
            pltpu.VMEM((2, half, batch, channels), bf),
            pltpu.VMEM((2, batch, channels), bf),
            pltpu.VMEM((2, batch, channels), bf),
            pltpu.VMEM((half, batch, 128), f32),
            pltpu.VMEM((half, batch, 128), f32),
            pltpu.VMEM((batch, 128), f32),
            pltpu.VMEM((batch, 128), f32),
            pltpu.VMEM((states, groups), f32),
            pltpu.VMEM((states, groups), f32),
            pltpu.VMEM((states, gs, groups), f32),
            pltpu.VMEM((states, gs, groups), f32),
            pltpu.VMEM((states, groups), f32),
            pltpu.VMEM((states, groups), f32),
            pltpu.VMEM((gs, states, groups), f32),
            pltpu.VMEM((gs, states, groups), f32),
            pltpu.VMEM((gs, states, groups), f32),
            pltpu.VMEM((gs, states, groups), f32),
            pltpu.VMEM((batch, states, groups), f32),
            pltpu.VMEM((batch, states, groups), f32),
            pltpu.VMEM((gs, gs, groups), f32),
            pltpu.VMEM((batch, gs, groups), f32),
            pltpu.VMEM((gs, batch, groups), f32),
            pltpu.VMEM((gs, batch, groups), f32),
            pltpu.VMEM((gs, batch, groups), f32),
            pltpu.VMEM((batch, gs, groups), f32),
            pltpu.VMEM((channels, batch), f32),
            pltpu.VMEM((channels, batch), f32),
            pltpu.VMEM((batch, channels), f32),
            pltpu.VMEM((batch, channels), bf),
            pltpu.VMEM((2, batch, channels), bf),
            pltpu.VMEM((channels, features // 2), bf),
            pltpu.VMEM((2 * batch, features // 2), f32),
            pltpu.VMEM((half * q, 2, batch, width), f32),
            pltpu.VMEM((half, 2, batch, width), bf),
            pltpu.VMEM((half, 2, batch, width), bf),
            pltpu.VMEM((half, 2, batch, width), bf),
            pltpu.VMEM((dp, 2, batch, width), bf),
            pltpu.VMEM((2, batch, width), f32),
            pltpu.VMEM((batch, width), f32),
            pltpu.VMEM((batch, width), f32),
            dma((2, q)),
            dma((dp,)),
            dma((dp,)),
            dma((dp,)),
            dma((dp,)),
            dma((3,)),
            dma((3,)),
            dma((3,)),
            dma((3,)),
            dma((8,)),
            dma((3,)),
            dma((2,)),
            dma,
            dma,
            dma((half, 2)),
            dma((half, 2)),
            dma((half, 2)),
            dma((dp, 2)),
            dma,
            dma,
        ],
        compiler_params=pltpu.CompilerParams(
            collective_id=ident, has_side_effects=True, vmem_limit_bytes=62 * 2**20
        ),
        name=f"layer_{layer}",
    )(*operands)


def on_device(
    tp,
    dp,
    tokens,
    gains,
    w_input,
    w_gating,
    w_output,
    decay_rate,
    frequency,
    log_step,
    in_real,
    in_imag,
    readout_real_matrix,
    readout_imag_matrix,
    skip_gain,
    state_real,
    state_imag,
):
    batch, width = tokens.shape
    groups, states = decay_rate.shape[1:]
    channels = groups * GS
    rows = w_input.shape[1]
    features = gains.shape[1]
    q = tp // dp
    d = lax.axis_index("dp")

    if q == 2 and dp == 4:
        eigen = (
            jnp.swapaxes(decay_rate, 1, 2),
            jnp.swapaxes(frequency, 1, 2),
            jnp.transpose(in_real, (0, 2, 3, 1)),
            jnp.transpose(in_imag, (0, 2, 3, 1)),
            jnp.transpose(readout_real_matrix, (0, 2, 3, 1)),
            jnp.transpose(readout_imag_matrix, (0, 2, 3, 1)),
        )
        state = (jnp.swapaxes(state_real, 2, 3), jnp.swapaxes(state_imag, 2, 3))
        gain = gains.reshape(LAYERS, tp, width)
        shard, news = tokens, ()
        for layer in range(LAYERS):
            before = shard
            shard, *news = layer_step(
                layer, shard, gain, skip_gain, w_input, w_gating, w_output,
                log_step, eigen, state, tuple(news), tp, dp, layer + 1,
            )
        shard = (before.astype(jnp.float32) + shard).astype(jnp.bfloat16)
        return shard, jnp.swapaxes(news[0], 2, 3), jnp.swapaxes(news[1], 2, 3)

    step = jnp.exp(log_step)[:, None, :]
    lam_re = -jnp.swapaxes(decay_rate, 1, 2)
    lam_im = jnp.swapaxes(frequency, 1, 2)
    magnitude = jnp.exp(lam_re * step)
    angle = lam_im * step
    abar_re = magnitude * jnp.cos(angle)
    abar_im = magnitude * jnp.sin(angle)
    denom = lam_re * lam_re + lam_im * lam_im
    num_re = abar_re - 1.0
    zoh_re = ((num_re * lam_re + abar_im * lam_im) / denom)[:, None]
    zoh_im = ((abar_im * lam_re - num_re * lam_im) / denom)[:, None]
    i_re = jnp.transpose(in_real, (0, 3, 2, 1))
    i_im = jnp.transpose(in_imag, (0, 3, 2, 1))
    bbar_re = zoh_re * i_re - zoh_im * i_im
    bbar_im = zoh_re * i_im + zoh_im * i_re
    r_re = jnp.transpose(readout_real_matrix, (0, 2, 3, 1))
    r_im = jnp.transpose(readout_imag_matrix, (0, 2, 3, 1))
    s_re = jnp.swapaxes(state_real, 2, 3)
    s_im = jnp.swapaxes(state_imag, 2, 3)
    my_gains = lax.dynamic_slice_in_dim(gains, d * rows, rows, 1).reshape(LAYERS, q, 1, width)

    shard = tokens
    news = ()
    for layer in range(LAYERS):
        got = gather(shard, tp, dp, 3 * layer + 1).reshape(q, dp * batch, width)
        xf = got.astype(jnp.float32)
        squares = jnp.sum(xf * xf, axis=(0, 2))
        scaled = (xf * my_gains[layer]).astype(jnp.bfloat16)
        if q <= 2:
            scaled = jnp.concatenate([scaled[h] for h in range(q)], axis=1)
        else:
            scaled = jnp.swapaxes(scaled, 0, 1).reshape(dp * batch, rows)
        drive = jnp.dot(scaled, w_input[layer], preferred_element_type=jnp.float32)
        gate = jnp.dot(scaled, w_gating[layer], preferred_element_type=jnp.float32)
        drive, gate, squares = exchange(
            [
                drive.astype(jnp.bfloat16).reshape(dp, batch, channels),
                gate.astype(jnp.bfloat16).reshape(dp, batch, channels),
                jnp.broadcast_to(squares.reshape(dp, batch, 1), (dp, batch, 128)),
            ],
            "dp",
            dp,
            3 * layer + 2,
        )
        meansq = jnp.sum(squares, axis=0)[:, :1] / features
        inverse = lax.rsqrt(meansq + 1e-06)
        drive = jnp.sum(drive.astype(jnp.float32), axis=0) * inverse
        gate = jnp.sum(gate.astype(jnp.float32), axis=0) * inverse
        u = jnp.swapaxes(drive.reshape(batch, groups, GS), 1, 2)
        n_re, n_im, y = state_step(
            layer, u, abar_re, abar_im, bbar_re, bbar_im, r_re, r_im, s_re, s_im, news
        )
        news = (n_re, n_im)
        y = jnp.swapaxes(y, 1, 2).reshape(batch, channels) + skip_gain[layer][None] * drive
        z = (jax.nn.gelu(y) * jax.nn.sigmoid(gate)).astype(jnp.bfloat16)
        branch = jnp.dot(z, w_output[layer], preferred_element_type=jnp.float32)
        pieces = jnp.swapaxes(branch.astype(jnp.bfloat16).reshape(batch, tp, width), 0, 1)
        (pieces,) = exchange([pieces], "tp", tp, 3 * layer + 3)
        summed = jnp.sum(pieces.astype(jnp.float32), axis=0)
        shard = (shard.astype(jnp.float32) + summed).astype(jnp.bfloat16)
    return shard, jnp.swapaxes(news[0], 2, 3), jnp.swapaxes(news[1], 2, 3)


def solution(mesh):
    placed = (
        P("dp", "tp"),
        P(),
        P(None, "dp", "tp"),
        P(None, "dp", "tp"),
        P(None, "tp", None),
        P(None, "tp", None),
        P(None, "tp", None),
        P(None, "tp"),
        P(None, "tp", None, None),
        P(None, "tp", None, None),
        P(None, "tp", None, None),
        P(None, "tp", None, None),
        P(None, "tp"),
        P(None, "dp", "tp", None),
        P(None, "dp", "tp", None),
    )
    return jax.shard_map(
        functools.partial(on_device, mesh.shape["tp"], mesh.shape["dp"]),
        mesh=mesh,
        in_specs=placed,
        out_specs=(P("dp", "tp"), P(None, "dp", "tp", None), P(None, "dp", "tp", None)),
        check_vma=False,
    )
```

```python
import functools

import jax
import jax.numpy as jnp
from jax import lax
from jax.experimental import pallas as pl
from jax.experimental.pallas import tpu as pltpu
from jax.sharding import PartitionSpec as P

GS = 16
LAYERS = 2
MESH = pl.DeviceIdType.MESH
ANY = pl.BlockSpec(memory_space=pl.ANY)


def exchange_kernel(axis, n, count, *refs):
    ins, outs = refs[:count], refs[count : 2 * count]
    send, recv, local = refs[2 * count :]
    me = lax.axis_index(axis)
    barrier = pltpu.get_barrier_semaphore()
    for i in range(1, n):
        pl.semaphore_signal(
            barrier, inc=1, device_id={axis: lax.rem(me + i, n)}, device_id_type=MESH
        )
    own = [
        pltpu.make_async_copy(ins[k].at[me], outs[k].at[me], local.at[k]) for k in range(count)
    ]
    for copy in own:
        copy.start()
    pl.semaphore_wait(barrier, n - 1)
    copies = []
    for i in range(1, n):
        peer = lax.rem(me + i, n)
        for k in range(count):
            copy = pltpu.make_async_remote_copy(
                src_ref=ins[k].at[peer],
                dst_ref=outs[k].at[me],
                send_sem=send.at[k, i],
                recv_sem=recv.at[k, i],
                device_id={axis: peer},
                device_id_type=MESH,
            )
            copy.start()
            copies.append((i, k, copy))
    for copy in own:
        copy.wait()
    for i, k, copy in copies:
        copy.wait_send()
        source = lax.rem(me + n - i, n)
        pltpu.make_async_remote_copy(
            src_ref=ins[k].at[source],
            dst_ref=outs[k].at[source],
            send_sem=send.at[k, i],
            recv_sem=recv.at[k, i],
            device_id={axis: source},
            device_id_type=MESH,
        ).wait_recv()


def exchange(arrays, axis, n, ident):
    count = len(arrays)
    return pl.pallas_call(
        functools.partial(exchange_kernel, axis, n, count),
        out_shape=[jax.ShapeDtypeStruct(a.shape, a.dtype) for a in arrays],
        in_specs=[ANY] * count,
        out_specs=[ANY] * count,
        scratch_shapes=[
            pltpu.SemaphoreType.DMA((count, n)),
            pltpu.SemaphoreType.DMA((count, n)),
            pltpu.SemaphoreType.DMA((count,)),
        ],
        compiler_params=pltpu.CompilerParams(collective_id=ident, has_side_effects=True),
        name=f"exchange_{axis}_{ident}",
    )(*arrays)


def gather_kernel(tp, dp, x_ref, out_ref, send, recv):
    q = tp // dp
    t = lax.axis_index("tp")
    d = lax.axis_index("dp")
    group = t // q
    slot = lax.rem(t, q) * dp + d
    barrier = pltpu.get_barrier_semaphore()
    for h in range(q):
        for r in range(dp):
            source = d * q + h
            pl.semaphore_signal(
                barrier, inc=1, device_id={"tp": source, "dp": r}, device_id_type=MESH
            )

    pl.semaphore_wait(barrier, tp)

    def remote(i, index):
        return pltpu.make_async_remote_copy(
            src_ref=x_ref,
            dst_ref=out_ref.at[index],
            send_sem=send.at[i],
            recv_sem=recv.at[index],
            device_id={"tp": lax.rem(t + i, tp), "dp": group},
            device_id_type=MESH,
        )

    home = group == d

    @pl.when(home)
    def _():
        pltpu.make_async_copy(x_ref, out_ref.at[slot], recv.at[slot]).start()

    @pl.when(jnp.logical_not(home))
    def _():
        remote(0, slot).start()

    for i in range(1, tp):
        remote(i, slot).start()
    for i in range(1, tp):
        remote(i, slot).wait_send()

    @pl.when(jnp.logical_not(home))
    def _():
        remote(0, slot).wait_send()

    for index in range(tp):
        pltpu.make_async_copy(x_ref, out_ref.at[index], recv.at[index]).wait()


def gather(x, tp, dp, ident):
    return pl.pallas_call(
        functools.partial(gather_kernel, tp, dp),
        out_shape=jax.ShapeDtypeStruct((tp,) + x.shape, x.dtype),
        in_specs=[ANY],
        out_specs=ANY,
        scratch_shapes=[pltpu.SemaphoreType.DMA((tp,)), pltpu.SemaphoreType.DMA((tp,))],
        compiler_params=pltpu.CompilerParams(collective_id=ident, has_side_effects=True),
        name=f"gather_{ident}",
    )(x)


def state_kernel(many, u_ref, are_ref, aim_ref, bre_ref, bim_ref, rre_ref, rim_ref, sre_ref, sim_ref, *rest):
    nre_ref, nim_ref, y_ref = rest[-3:]
    block, channels = u_ref.shape[0], u_ref.shape[1]
    states = are_ref.shape[1]
    cut = 4

    def body(step, carry):
        first = step * many
        for p in range(0, states, 8):
            rows = slice(p, p + 8)
            a_re, a_im = are_ref[0, rows, :], aim_ref[0, rows, :]
            new_re, new_im = [], []
            for b in range(many):
                o_re, o_im = sre_ref[0, first + b, rows, :], sim_ref[0, first + b, rows, :]
                new_re.append(a_re * o_re - a_im * o_im)
                new_im.append(a_re * o_im + a_im * o_re)
            for c in range(channels):
                b_re, b_im = bre_ref[0, c, rows, :], bim_ref[0, c, rows, :]
                for b in range(many):
                    u = u_ref[first + b, c : c + 1, :]
                    new_re[b] = new_re[b] + b_re * u
                    new_im[b] = new_im[b] + b_im * u
            for b in range(many):
                nre_ref[0, first + b, rows, :] = new_re[b]
                nim_ref[0, first + b, rows, :] = new_im[b]
        for c in range(0, channels, cut):
            total = [[None] * many for _ in range(cut)]
            for p in range(0, states, 8):
                rows = slice(p, p + 8)
                h_re = [nre_ref[0, first + b, rows, :] for b in range(many)]
                h_im = [nim_ref[0, first + b, rows, :] for b in range(many)]
                for j in range(cut):
                    r_re, r_im = rre_ref[0, c + j, rows, :], rim_ref[0, c + j, rows, :]
                    for b in range(many):
                        term = r_re * h_re[b] - r_im * h_im[b]
                        total[j][b] = term if p == 0 else total[j][b] + term
            for j in range(cut):
                for b in range(many):
                    y_ref[first + b, c + j : c + j + 1, :] = jnp.sum(
                        total[j][b], axis=0, keepdims=True
                    )
        return carry

    lax.fori_loop(0, block // many, body, 0)


def state_step(layer, u, a_re, a_im, b_re, b_im, r_re, r_im, s_re, s_im, earlier):
    batch, channels, groups = u.shape
    states = a_re.shape[1]
    block = 8
    per_batch = pl.BlockSpec((block, channels, groups), lambda i: (i, 0, 0))
    eigen = pl.BlockSpec((1, states, groups), lambda i: (layer, 0, 0))
    matrix = pl.BlockSpec((1, channels, states, groups), lambda i: (layer, 0, 0, 0))
    state = pl.BlockSpec((1, block, states, groups), lambda i: (layer, i, 0, 0))
    specs = [per_batch, eigen, eigen, matrix, matrix, matrix, matrix, state, state]
    aliases = {}
    if earlier:
        aliases = {len(specs): 0, len(specs) + 1: 1}
    return pl.pallas_call(
        functools.partial(state_kernel, 4),
        grid=(batch // block,),
        out_shape=[
            jax.ShapeDtypeStruct(s_re.shape, jnp.float32),
            jax.ShapeDtypeStruct(s_im.shape, jnp.float32),
            jax.ShapeDtypeStruct(u.shape, jnp.float32),
        ],
        in_specs=specs + [ANY] * len(earlier),
        out_specs=[state, state, per_batch],
        input_output_aliases=aliases,
        name=f"state_{layer}",
    )(u, a_re, a_im, b_re, b_im, r_re, r_im, s_re, s_im, *earlier)


def remote(src, dst, send, recv, target):
    return pltpu.make_async_remote_copy(
        src_ref=src,
        dst_ref=dst,
        send_sem=send,
        recv_sem=recv,
        device_id=target,
        device_id_type=MESH,
    )


def greet(barrier, target):
    pl.semaphore_signal(barrier, inc=1, device_id=target, device_id_type=MESH)


def layer_kernel(
    layer, tp, dp, features, earlier,
    x_ref, gain_ref, skip_ref, win_ref, wgate_ref, wout_ref,
    logstep_ref, decay_ref, freq_ref, ire_ref, iim_ref, rre_ref, rim_ref, sre_ref, sim_ref,
    *rest,
):
    out_ref, nre_ref, nim_ref = rest[earlier : earlier + 3]
    (
        xg, wbuf, scaled, acc, squares,
        out1, in1, out2, in2, sq_out1, sq_in1, sq_out2, sq_in2,
        gain_rows, decay, freq, i_re, i_im,
        a_re, a_im, b_re, b_im, r_re, r_im, h_re, h_im,
        mix, y0, y0p, y3, u3, ub, flip, flipy, unat, gated,
        both, wobuf, prod, blocks, ybuf, yin, zbuf, zin, own, last, last_in,
        wsem, gsend, grecv, across_send, across_recv, send1, recv1, send2, recv2,
        ssem, osem, psem, swap_send, swap_recv, ysend, yrecv, zsend, zrecv, fsend, frecv,
    ) = rest[earlier + 3 :]
    q = tp // dp
    half = dp // 2
    t, d = lax.axis_index("tp"), lax.axis_index("dp")
    z, y = t // q, t % q
    x, c = d // 2, d % 2
    home = z == d
    batch, width = x_ref.shape
    channels = unat.shape[1]
    states, groups = a_re.shape
    gs = channels // groups
    partner = 2 * x + 1 - c
    far = (d + 2) % dp
    beside = 2 * (far // 2) + 1 - far % 2
    other = 1 - y
    collects = z // half == c
    columns = wobuf.shape[1]
    pieces = 3
    piece = columns // pieces

    params = [
        pltpu.make_async_copy(src.at[layer], dst, ssem.at[i])
        for i, (src, dst) in enumerate(
            (
                (decay_ref, decay), (freq_ref, freq), (ire_ref, i_re), (iim_ref, i_im),
                (rre_ref, r_re), (rim_ref, r_im), (sre_ref, h_re), (sim_ref, h_im),
            )
        )
    ]
    for copy in params:
        copy.start()
    def fetch(n):
        return pltpu.make_async_copy(
            wout_ref.at[layer, :, pl.ds(pl.multiple_of(c * columns + n * piece, 128), piece)],
            wobuf.at[:, pl.ds(n * piece, piece)],
            osem.at[n],
        )

    barrier = pltpu.get_barrier_semaphore()
    for e in range(dp):
        @pl.when(jnp.logical_not(jnp.logical_and(home, d == e)))
        def _():
            greet(barrier, {"tp": d * q + y, "dp": e})
    greet(barrier, {"tp": z * q + other})
    greet(barrier, {"dp": partner})
    greet(barrier, {"dp": far})

    @pl.when(collects)
    def _():
        for o in range(1, dp):
            greet(barrier, {"tp": ((z + o) % dp) * q + y})

    pl.semaphore_wait(
        barrier, dp + 3 + half - home.astype(jnp.int32) - collects.astype(jnp.int32)
    )

    upper = z // half
    order = [
        (dp - 1) * (1 - upper),
        half - upper,
        z + 1 - 2 * (z % 2),
        z,
    ]

    def spread(i):
        return remote(
            x_ref, xg.at[y, d], gsend.at[i], grecv.at[d], {"tp": order[i] * q + y, "dp": z}
        )

    for i in range(dp - 1):
        spread(i).start()

    @pl.when(home)
    def _():
        xg[y, d] = x_ref[...]

    @pl.when(jnp.logical_not(home))
    def _():
        spread(dp - 1).start()

    def across(src, e, slot):
        return remote(
            src, xg.at[slot, e], across_send.at[e], across_recv.at[e], {"tp": z * q + other}
        )

    slots = [d, partner, far, beside]
    many, cut = 4, 4

    def mixing(o, carry):
        for i in range(0, gs, cut):
            total = [None] * cut
            for p in range(0, states, 8):
                rows = slice(p, p + 8)
                left_re, left_im = r_re[o, rows, :], r_im[o, rows, :]
                for j in range(cut):
                    term = left_re * b_re[i + j, rows, :] - left_im * b_im[i + j, rows, :]
                    total[j] = term if p == 0 else total[j] + term
            for j in range(cut):
                mix[o, i + j : i + j + 1, :] = jnp.sum(total[j], axis=0, keepdims=True)
        return carry

    def recall(step, carry):
        first = step * many
        for p in range(0, states, 8):
            rows = slice(p, p + 8)
            pole_re, pole_im = a_re[rows, :], a_im[rows, :]
            for b in range(many):
                o_re, o_im = h_re[first + b, rows, :], h_im[first + b, rows, :]
                h_re[first + b, rows, :] = pole_re * o_re - pole_im * o_im
                h_im[first + b, rows, :] = pole_re * o_im + pole_im * o_re
        for i in range(0, gs, cut):
            total = [[None] * many for _ in range(cut)]
            for p in range(0, states, 8):
                rows = slice(p, p + 8)
                n_re = [h_re[first + b, rows, :] for b in range(many)]
                n_im = [h_im[first + b, rows, :] for b in range(many)]
                for j in range(cut):
                    left_re, left_im = r_re[i + j, rows, :], r_im[i + j, rows, :]
                    for b in range(many):
                        term = left_re * n_re[b] - left_im * n_im[b]
                        total[j][b] = term if p == 0 else total[j][b] + term
            for j in range(cut):
                for b in range(many):
                    y0[first + b, i + j : i + j + 1, :] = jnp.sum(
                        total[j][b], axis=0, keepdims=True
                    )
        return carry

    def push(step, carry):
        first = step * many
        for p in range(0, states, 8):
            rows = slice(p, p + 8)
            n_re = [h_re[first + b, rows, :] for b in range(many)]
            n_im = [h_im[first + b, rows, :] for b in range(many)]
            for i in range(gs):
                in_re, in_im = b_re[i, rows, :], b_im[i, rows, :]
                for b in range(many):
                    u = ub[first + b, i : i + 1, :]
                    n_re[b] = n_re[b] + in_re * u
                    n_im[b] = n_im[b] + in_im * u
            for b in range(many):
                h_re[first + b, rows, :] = n_re[b]
                h_im[first + b, rows, :] = n_im[b]
        return carry

    for j in range(tp):
        gain_rows[j] = gain_ref[layer : layer + 1, j * width : (j + 1) * width]
    for copy in params[:4]:
        copy.wait()
    step = jnp.exp(logstep_ref[layer : layer + 1, :])
    lam_re, lam_im = -decay[...], freq[...]
    magnitude = jnp.exp(lam_re * step)
    angle = lam_im * step
    pole_re, pole_im = magnitude * jnp.cos(angle), magnitude * jnp.sin(angle)
    denom = lam_re * lam_re + lam_im * lam_im
    num_re = pole_re - 1.0
    a_re[...] = pole_re
    a_im[...] = pole_im
    zoh_re = (num_re * lam_re + pole_im * lam_im) / denom
    zoh_im = (pole_im * lam_re - num_re * lam_im) / denom
    flat_re, flat_im = i_re.reshape(states * gs, groups), i_im.reshape(states * gs, groups)
    for i in range(gs):
        col = pl.ds(i, states, stride=gs)
        in_re, in_im = flat_re[col, :], flat_im[col, :]
        b_re[i] = zoh_re * in_re - zoh_im * in_im
        b_im[i] = zoh_re * in_im + zoh_im * in_re
    for copy in params[4:]:
        copy.wait()
    for m, w in enumerate((win_ref, wgate_ref)):
        for h in range(q):
            pltpu.make_async_copy(
                w.at[layer, pl.ds(h * width, width), :], wbuf.at[m, h], wsem.at[m, h]
            ).start()
    lax.fori_loop(0, gs, mixing, 0)
    steps = batch // many
    marks = [(i * steps) // dp for i in range(dp + 1)]
    for i in range(dp):
        lax.fori_loop(marks[i], marks[i + 1], recall, 0)
        e = slots[i]
        if i == 0:
            @pl.when(home)
            def _():
                across(x_ref, e, y).start()

            @pl.when(jnp.logical_not(home))
            def _():
                remote(x_ref, xg.at[y, e], gsend.at[0], grecv.at[e], {"dp": partner}).wait_recv()
                across(xg.at[y, e], e, y).start()
        else:
            remote(x_ref, xg.at[y, e], gsend.at[0], grecv.at[e], {"dp": partner}).wait_recv()
            across(xg.at[y, e], e, y).start()

    def scale(h, first):
        gain = gain_rows[d * q + h]
        for e in range(dp):
            xf = xg[h, e].astype(jnp.float32)
            total = jnp.broadcast_to(jnp.sum(xf * xf, axis=1, keepdims=True), squares.shape[1:])
            squares[e] = total if first else squares[e] + total
            scaled[e * batch : (e + 1) * batch, :] = (xf * gain).astype(jnp.bfloat16)

    tile = channels

    scale(y, True)
    for m in range(2):
        pltpu.make_async_copy(
            win_ref.at[layer, pl.ds(0, width), :], wbuf.at[m, y], wsem.at[m, y]
        ).wait()

        def first(n, carry):
            cols = pl.ds(pl.multiple_of(n * tile, 128), tile)
            part = jnp.dot(scaled[...], wbuf[m, y, :, cols], preferred_element_type=jnp.float32)
            acc[m, :, :, cols] = part.reshape(dp, batch, tile)
            return carry

        lax.fori_loop(0, channels // tile, first, 0)

    for n in range(pieces):
        fetch(n).start()
    flat = y0.reshape(batch * gs, groups)
    for i in range(gs):
        y0p[i] = flat[pl.ds(i, batch, stride=gs), :]

    for i in range(dp):
        across(x_ref, slots[i], other).wait_recv()
    scale(other, False)
    for h in range(half):
        sq_out1[h] = squares[2 * h + 1 - c]
    sq1 = remote(sq_out1, sq_in1, send1.at[2], recv1.at[2], {"dp": partner})
    sq1.start()

    def stage1(m):
        return remote(out1.at[m], in1.at[m], send1.at[m], recv1.at[m], {"dp": partner})

    def stage2(m):
        return remote(out2.at[m], in2.at[m], send2.at[m], recv2.at[m], {"dp": far})

    for m in range(2):
        pltpu.make_async_copy(
            win_ref.at[layer, pl.ds(0, width), :], wbuf.at[m, other], wsem.at[m, other]
        ).wait()

        def second(n, carry):
            cols = pl.ds(pl.multiple_of(n * tile, 128), tile)
            part = jnp.dot(
                scaled[...], wbuf[m, other, :, cols], preferred_element_type=jnp.float32
            )
            acc[m, :, :, cols] = acc[m, :, :, cols] + part.reshape(dp, batch, tile)
            for h in range(half):
                out1[m, h, :, cols] = acc[m, 2 * h + 1 - c, :, cols].astype(jnp.bfloat16)
            return carry

        lax.fori_loop(0, channels // tile, second, 0)
        stage1(m).start()

    sq1.wait()
    sq_out2[...] = squares[far] + sq_in1[1 - x]
    sq2 = remote(sq_out2, sq_in2, send2.at[2], recv2.at[2], {"dp": far})
    sq2.start()
    for m in range(2):
        stage1(m).wait()
        out2[m] = (acc[m, far] + in1[m, 1 - x].astype(jnp.float32)).astype(jnp.bfloat16)
        stage2(m).start()
        acc[m, d] = acc[m, d] + in1[m, x].astype(jnp.float32)
    sq2.wait()
    meansq = (squares[d] + sq_in1[x] + sq_in2[...])[:, :1] / features
    inverse = lax.rsqrt(meansq + 1e-06)
    stage2(0).wait()
    drive = (acc[0, d] + in2[0].astype(jnp.float32)) * inverse
    unat[...] = drive
    flip[...] = drive.T
    for i in range(gs):
        u3[i] = flip[pl.ds(i, groups, stride=gs), :].T

    def respond(n, carry):
        rows = pl.ds(pl.multiple_of(n * 8, 8), 8)
        u = [u3[i, rows, :] for i in range(gs)]
        for o in range(gs):
            total = y0p[o, rows, :]
            for i in range(gs):
                total = total + mix[o, i : i + 1, :] * u[i]
            y3[o, rows, :] = total
        return carry

    lax.fori_loop(0, batch // 8, respond, 0)
    for i in range(gs):
        flipy[pl.ds(i, groups, stride=gs), :] = y3[i].T
    read = flipy[...].T + skip_ref[layer : layer + 1, :] * unat[...]
    stage2(1).wait()
    gate = (acc[1, d] + in2[1].astype(jnp.float32)) * inverse
    gated[...] = (jax.nn.gelu(read) * jax.nn.sigmoid(gate)).astype(jnp.bfloat16)

    swap = remote(gated, both.at[c], swap_send, swap_recv, {"dp": partner})
    swap.start()
    both[c] = gated[...]
    flat_u = u3.reshape(gs * batch, groups)
    for b in range(batch):
        ub[b] = flat_u[pl.ds(b, gs, stride=batch), :]
    remote(gated, both.at[1 - c], swap_send, swap_recv, {"dp": partner}).wait_recv()
    first_turn = jnp.where(c == 0, jnp.where(z == 0, 1, 0), jnp.where(z == dp - 1, 0, 1))
    turns = [first_turn, 1 - first_turn]

    def over_y(k, e):
        return remote(
            ybuf.at[k, e], yin.at[k, e], ysend.at[k, e], yrecv.at[k, e], {"tp": z * q + other}
        )

    def over_z(k, e):
        return remote(
            zbuf.at[k, e],
            zin.at[z, e],
            zsend.at[k, e],
            zrecv.at[z, e],
            {"tp": (half * c + k) * q + y},
        )

    rows = both[...].reshape(2 * batch, channels)

    def multiply(n):
        pltpu.make_async_copy(
            wout_ref.at[layer, :, pl.ds(0, piece)], wobuf.at[:, pl.ds(0, piece)], osem.at[n]
        ).wait()
        span = pl.ds(pl.multiple_of(n * piece, 128), piece)
        prod[:, span] = jnp.dot(rows, wobuf[:, span], preferred_element_type=jnp.float32)

    def send_over_y(k):
        for static in range(half):
            @pl.when(k == static)
            def _():
                for j in range(static * q, (static + 1) * q):
                    for e in range(2):
                        blocks[j, e] = prod[
                            e * batch : (e + 1) * batch, j * width : (j + 1) * width
                        ]
        for e in range(2):
            ybuf[k, e] = blocks[q * k + other, e].astype(jnp.bfloat16)
            over_y(k, e).start()

    multiply((pieces - 1) * first_turn)
    multiply(1)
    send_over_y(turns[0])
    multiply((pieces - 1) * turns[1])
    send_over_y(turns[1])
    results = [
        pltpu.make_async_copy(h_re, nre_ref.at[layer], psem.at[0]),
        pltpu.make_async_copy(h_im, nim_ref.at[layer], psem.at[1]),
    ]
    early = 2 * steps // 3
    for i, k in enumerate(turns):
        mine = half * c + k == z
        for e in range(2):
            if i == 0:
                lax.fori_loop(e * early, steps if e else early, push, 0)
                if e:
                    for copy in results:
                        copy.start()
            over_y(k, e).wait_recv()
            total = blocks[q * k + y, e] + yin[k, e].astype(jnp.float32)

            @pl.when(mine)
            def _():
                own[e] = total

            @pl.when(jnp.logical_not(mine))
            def _():
                zbuf[k, e] = total.astype(jnp.bfloat16)
                over_z(k, e).start()

    def finish(total):
        if layer == LAYERS - 1:
            out_ref[...] = total
        else:
            out_ref[...] = (x_ref[...].astype(jnp.float32) + total).astype(jnp.bfloat16)

    final = remote(last, last_in, fsend, frecv, {"dp": partner})

    def gathered(e):
        total = own[e]
        for o in range(1, dp):
            source = (z + o) % dp
            remote(
                zbuf.at[0, 0], zin.at[source, e], zsend.at[0, 0], zrecv.at[source, e],
                {"dp": partner},
            ).wait_recv()
            total = total + zin[source, e].astype(jnp.float32)
        return total

    @pl.when(collects)
    def _():
        last[...] = gathered(1 - c)
        final.start()
        finish(gathered(c))
        final.wait_send()

    @pl.when(jnp.logical_not(collects))
    def _():
        final.wait_recv()
        finish(last_in[...])

    for copy in results:
        copy.wait()
    for i in range(dp - 1):
        spread(i).wait_send()

    @pl.when(jnp.logical_not(home))
    def _():
        spread(dp - 1).wait_send()

    for i in range(dp):
        across(x_ref, slots[i], y).wait_send()
    swap.wait_send()
    for k in range(2):
        for e in range(2):
            over_y(k, e).wait_send()

            @pl.when(half * c + k != z)
            def _():
                over_z(k, e).wait_send()


def layer_step(
    layer, x, gain, skip, w_input, w_gating, w_output, log_step, eigen, state, earlier, tp, dp, ident
):
    batch, width = x.shape
    channels = w_input.shape[2]
    states, groups = eigen[0].shape[1:]
    gs = channels // groups
    features = w_output.shape[2]
    q = tp // dp
    half = dp // 2
    bf, f32 = jnp.bfloat16, jnp.float32
    vmem = pl.BlockSpec(memory_space=pltpu.VMEM)
    dma = pltpu.SemaphoreType.DMA
    operands = [
        x, gain, skip, w_input, w_gating, w_output, log_step, *eigen, *state, *earlier
    ]
    aliases = {len(operands) - 2: 1, len(operands) - 1: 2} if earlier else {}
    return pl.pallas_call(
        functools.partial(layer_kernel, layer, tp, dp, features, len(earlier)),
        out_shape=[jax.ShapeDtypeStruct((batch, width), f32 if layer == LAYERS - 1 else bf)]
        + [jax.ShapeDtypeStruct(a.shape, f32) for a in state],
        in_specs=[vmem] * 3 + [ANY] * 3 + [vmem] + [ANY] * (len(operands) - 7),
        out_specs=[vmem, ANY, ANY],
        input_output_aliases=aliases,
        scratch_shapes=[
            pltpu.VMEM((q, dp, batch, width), bf),
            pltpu.VMEM((2, q, width, channels), bf),
            pltpu.VMEM((dp * batch, width), bf),
            pltpu.VMEM((2, dp, batch, channels), f32),
            pltpu.VMEM((dp, batch, 128), f32),
            pltpu.VMEM((2, half, batch, channels), bf),
            pltpu.VMEM((2, half, batch, channels), bf),
            pltpu.VMEM((2, batch, channels), bf),
            pltpu.VMEM((2, batch, channels), bf),
            pltpu.VMEM((half, batch, 128), f32),
            pltpu.VMEM((half, batch, 128), f32),
            pltpu.VMEM((batch, 128), f32),
            pltpu.VMEM((batch, 128), f32),
            pltpu.VMEM((tp, 1, width), f32),
            pltpu.VMEM((states, groups), f32),
            pltpu.VMEM((states, groups), f32),
            pltpu.VMEM((states, gs, groups), f32),
            pltpu.VMEM((states, gs, groups), f32),
            pltpu.VMEM((states, groups), f32),
            pltpu.VMEM((states, groups), f32),
            pltpu.VMEM((gs, states, groups), f32),
            pltpu.VMEM((gs, states, groups), f32),
            pltpu.VMEM((gs, states, groups), f32),
            pltpu.VMEM((gs, states, groups), f32),
            pltpu.VMEM((batch, states, groups), f32),
            pltpu.VMEM((batch, states, groups), f32),
            pltpu.VMEM((gs, gs, groups), f32),
            pltpu.VMEM((batch, gs, groups), f32),
            pltpu.VMEM((gs, batch, groups), f32),
            pltpu.VMEM((gs, batch, groups), f32),
            pltpu.VMEM((gs, batch, groups), f32),
            pltpu.VMEM((batch, gs, groups), f32),
            pltpu.VMEM((channels, batch), f32),
            pltpu.VMEM((channels, batch), f32),
            pltpu.VMEM((batch, channels), f32),
            pltpu.VMEM((batch, channels), bf),
            pltpu.VMEM((2, batch, channels), bf),
            pltpu.VMEM((channels, features // 2), bf),
            pltpu.VMEM((2 * batch, features // 2), f32),
            pltpu.VMEM((half * q, 2, batch, width), f32),
            pltpu.VMEM((half, 2, batch, width), bf),
            pltpu.VMEM((half, 2, batch, width), bf),
            pltpu.VMEM((half, 2, batch, width), bf),
            pltpu.VMEM((dp, 2, batch, width), bf),
            pltpu.VMEM((2, batch, width), f32),
            pltpu.VMEM((batch, width), f32),
            pltpu.VMEM((batch, width), f32),
            dma((2, q)),
            dma((dp,)),
            dma((dp,)),
            dma((dp,)),
            dma((dp,)),
            dma((3,)),
            dma((3,)),
            dma((3,)),
            dma((3,)),
            dma((8,)),
            dma((3,)),
            dma((2,)),
            dma,
            dma,
            dma((half, 2)),
            dma((half, 2)),
            dma((half, 2)),
            dma((dp, 2)),
            dma,
            dma,
        ],
        compiler_params=pltpu.CompilerParams(
            collective_id=ident, has_side_effects=True, vmem_limit_bytes=62 * 2**20
        ),
        name=f"layer_{layer}",
    )(*operands)


def finish_kernel(
    sum_ref, x_ref, re_ref, im_ref, out_ref, nre_ref, nim_ref,
    total, x, mixed, held, rsem, wsem, small,
):
    layers, batch = re_ref.shape[:2]
    pieces = rsem.shape[2]
    size = batch // pieces
    moves = []
    for n in range(pieces):
        for layer in range(layers):
            for i, (src, dst) in enumerate(((re_ref, nre_ref), (im_ref, nim_ref))):
                part = (layer, pl.ds(n * size, size))
                take = pltpu.make_async_copy(
                    src.at[part], held.at[i].at[part], rsem.at[i, layer, n]
                )
                take.start()
                put = pltpu.make_async_copy(
                    held.at[i].at[part], dst.at[part], wsem.at[i, layer, n]
                )
                moves.append((take, put))
    loads = [
        pltpu.make_async_copy(sum_ref, total, small.at[0]),
        pltpu.make_async_copy(x_ref, x, small.at[1]),
    ]
    for copy in loads:
        copy.start()
    for take, put in moves:
        take.wait()
        put.start()
    for copy in loads:
        copy.wait()
    mixed[...] = (x[...].astype(jnp.float32) + total[...]).astype(jnp.bfloat16)
    result = pltpu.make_async_copy(mixed, out_ref, small.at[2])
    result.start()
    for take, put in moves:
        put.wait()
    result.wait()


def finish(total, x, n_re, n_im):
    pieces = 4
    return pl.pallas_call(
        finish_kernel,
        out_shape=[jax.ShapeDtypeStruct(a.shape, a.dtype) for a in (x, n_re, n_im)],
        in_specs=[ANY] * 4,
        out_specs=[ANY] * 3,
        scratch_shapes=[
            pltpu.VMEM(total.shape, total.dtype),
            pltpu.VMEM(x.shape, x.dtype),
            pltpu.VMEM(x.shape, x.dtype),
            pltpu.VMEM((2,) + n_re.shape, n_re.dtype),
            pltpu.SemaphoreType.DMA((2, n_re.shape[0], pieces)),
            pltpu.SemaphoreType.DMA((2, n_re.shape[0], pieces)),
            pltpu.SemaphoreType.DMA((3,)),
        ],
        compiler_params=pltpu.CompilerParams(vmem_limit_bytes=62 * 2**20),
        name="finish",
    )(total, x, n_re, n_im)


def on_device(
    tp,
    dp,
    tokens,
    gains,
    w_input,
    w_gating,
    w_output,
    decay_rate,
    frequency,
    log_step,
    in_real,
    in_imag,
    readout_real_matrix,
    readout_imag_matrix,
    skip_gain,
    state_real,
    state_imag,
):
    batch, width = tokens.shape
    groups, states = decay_rate.shape[1:]
    channels = groups * GS
    rows = w_input.shape[1]
    features = gains.shape[1]
    q = tp // dp
    d = lax.axis_index("dp")

    if q == 2 and dp == 4:
        eigen = (
            jnp.swapaxes(decay_rate, 1, 2),
            jnp.swapaxes(frequency, 1, 2),
            jnp.transpose(in_real, (0, 2, 3, 1)),
            jnp.transpose(in_imag, (0, 2, 3, 1)),
            jnp.transpose(readout_real_matrix, (0, 2, 3, 1)),
            jnp.transpose(readout_imag_matrix, (0, 2, 3, 1)),
        )
        state = (jnp.swapaxes(state_real, 2, 3), jnp.swapaxes(state_imag, 2, 3))
        shard, news = tokens, ()
        for layer in range(LAYERS):
            before = shard
            shard, *news = layer_step(
                layer, shard, gains, skip_gain, w_input, w_gating, w_output,
                log_step, eigen, state, tuple(news), tp, dp, layer + 1,
            )
        shard, *news = finish(shard, before, *news)
        return shard, jnp.swapaxes(news[0], 2, 3), jnp.swapaxes(news[1], 2, 3)

    step = jnp.exp(log_step)[:, None, :]
    lam_re = -jnp.swapaxes(decay_rate, 1, 2)
    lam_im = jnp.swapaxes(frequency, 1, 2)
    magnitude = jnp.exp(lam_re * step)
    angle = lam_im * step
    abar_re = magnitude * jnp.cos(angle)
    abar_im = magnitude * jnp.sin(angle)
    denom = lam_re * lam_re + lam_im * lam_im
    num_re = abar_re - 1.0
    zoh_re = ((num_re * lam_re + abar_im * lam_im) / denom)[:, None]
    zoh_im = ((abar_im * lam_re - num_re * lam_im) / denom)[:, None]
    i_re = jnp.transpose(in_real, (0, 3, 2, 1))
    i_im = jnp.transpose(in_imag, (0, 3, 2, 1))
    bbar_re = zoh_re * i_re - zoh_im * i_im
    bbar_im = zoh_re * i_im + zoh_im * i_re
    r_re = jnp.transpose(readout_real_matrix, (0, 2, 3, 1))
    r_im = jnp.transpose(readout_imag_matrix, (0, 2, 3, 1))
    s_re = jnp.swapaxes(state_real, 2, 3)
    s_im = jnp.swapaxes(state_imag, 2, 3)
    my_gains = lax.dynamic_slice_in_dim(gains, d * rows, rows, 1).reshape(LAYERS, q, 1, width)

    shard = tokens
    news = ()
    for layer in range(LAYERS):
        got = gather(shard, tp, dp, 3 * layer + 1).reshape(q, dp * batch, width)
        xf = got.astype(jnp.float32)
        squares = jnp.sum(xf * xf, axis=(0, 2))
        scaled = (xf * my_gains[layer]).astype(jnp.bfloat16)
        if q <= 2:
            scaled = jnp.concatenate([scaled[h] for h in range(q)], axis=1)
        else:
            scaled = jnp.swapaxes(scaled, 0, 1).reshape(dp * batch, rows)
        drive = jnp.dot(scaled, w_input[layer], preferred_element_type=jnp.float32)
        gate = jnp.dot(scaled, w_gating[layer], preferred_element_type=jnp.float32)
        drive, gate, squares = exchange(
            [
                drive.astype(jnp.bfloat16).reshape(dp, batch, channels),
                gate.astype(jnp.bfloat16).reshape(dp, batch, channels),
                jnp.broadcast_to(squares.reshape(dp, batch, 1), (dp, batch, 128)),
            ],
            "dp",
            dp,
            3 * layer + 2,
        )
        meansq = jnp.sum(squares, axis=0)[:, :1] / features
        inverse = lax.rsqrt(meansq + 1e-06)
        drive = jnp.sum(drive.astype(jnp.float32), axis=0) * inverse
        gate = jnp.sum(gate.astype(jnp.float32), axis=0) * inverse
        u = jnp.swapaxes(drive.reshape(batch, groups, GS), 1, 2)
        n_re, n_im, y = state_step(
            layer, u, abar_re, abar_im, bbar_re, bbar_im, r_re, r_im, s_re, s_im, news
        )
        news = (n_re, n_im)
        y = jnp.swapaxes(y, 1, 2).reshape(batch, channels) + skip_gain[layer][None] * drive
        z = (jax.nn.gelu(y) * jax.nn.sigmoid(gate)).astype(jnp.bfloat16)
        branch = jnp.dot(z, w_output[layer], preferred_element_type=jnp.float32)
        pieces = jnp.swapaxes(branch.astype(jnp.bfloat16).reshape(batch, tp, width), 0, 1)
        (pieces,) = exchange([pieces], "tp", tp, 3 * layer + 3)
        summed = jnp.sum(pieces.astype(jnp.float32), axis=0)
        shard = (shard.astype(jnp.float32) + summed).astype(jnp.bfloat16)
    return shard, jnp.swapaxes(news[0], 2, 3), jnp.swapaxes(news[1], 2, 3)


def solution(mesh):
    placed = (
        P("dp", "tp"),
        P(),
        P(None, "dp", "tp"),
        P(None, "dp", "tp"),
        P(None, "tp", None),
        P(None, "tp", None),
        P(None, "tp", None),
        P(None, "tp"),
        P(None, "tp", None, None),
        P(None, "tp", None, None),
        P(None, "tp", None, None),
        P(None, "tp", None, None),
        P(None, "tp"),
        P(None, "dp", "tp", None),
        P(None, "dp", "tp", None),
    )
    return jax.shard_map(
        functools.partial(on_device, mesh.shape["tp"], mesh.shape["dp"]),
        mesh=mesh,
        in_specs=placed,
        out_specs=(P("dp", "tp"), P(None, "dp", "tp", None), P(None, "dp", "tp", None)),
        check_vma=False,
    )
```
